32 devices in a mesh: kv: 8 (over z, y), tp: 4 (over x, core).
Axes of the slice: x: 2, y: 2, z: 4, core: 2. Of those that a mesh axis runs over, the one named last changes fastest.
Arguments:
- queries: bfloat16 [2, 3072, 1024], P(None, 'kv', 'tp'), may hold values from -112 to 112
- key_states: bfloat16 [2, 3072, 256], P(None, 'kv', 'tp'), may hold values from -4 to 4
- value_states: bfloat16 [2, 3072, 256], P(None, 'kv', 'tp'), may hold values from -6 to 6
- cotangent: bfloat16 [2, 3072, 1024], P(None, 'kv', 'tp'), may hold values from -6 to 6
- gate_logits: float32 [2, 3072, 16], P(None, 'kv', 'tp'), may hold values from -6 to 6
- layer_input: bfloat16 [2, 3072, 4096], P(None, ('kv', 'tp')), may hold values from -6 to 6
- chosen: int32 [2, 48, 4, 16], P(None, 'kv', 'tp'), may hold values from 0 to 47, as said below
Outputs:
- query_grad: bfloat16 [2, 3072, 1024], P(None, 'kv', 'tp')
- key_grad: bfloat16 [2, 3072, 256], P(None, 'kv', 'tp')
- value_grad: bfloat16 [2, 3072, 256], P(None, 'kv', 'tp')
- value_weight_grad: float32 [4096, 256], P(('kv', 'tp'))
The draws below stay inside these ranges and needn't reach their ends.
Inputs may be any that keep to these rules, and one draw needn't show every extreme that they name: `chosen`: for each sequence, query block b and key head, the 16 entries are distinct blocks; they include b itself and block 0; blocks after b hold only keys after all of the block's queries. Taking the 6 query blocks of one index of kv together (aligned), one sequence and one key head, at most 2 distinct blocks held by any one earlier index of kv are named, and some index reaches 2.
All inputs are finite; a program needn't handle non-finite values.
Results may differ from the reference program's by a relative error of at most 0.0058.
Values may be sent and summed in bfloat16 or wider, within the bound.
No kernel may reach another device: no remote copies, remote signals or barrier semaphores. Data moves between devices by JAX's collectives and lax.ppermute only.
A program may use at most 128 MiB of HBM per device.

```python
import jax
import jax.numpy as jnp
from jax import lax

D = 4096
H = 16
KVH = 4
HD = 64
BLK = 64
TOPK = 16
MOST = 2
SEQS = 2
BPD = 6
SEQ = 3072
NBLK = 48
N_KV = 8


def key_field(key):
    drawn = jax.random.normal(jax.random.fold_in(key, 11), (SEQS, SEQ, KVH * HD), jnp.float32)
    return jnp.clip(drawn, -4.0, 4.0)


def draw_key_states(key, part):
    return key_field(key).astype(jnp.bfloat16)


def draw_queries(key, part):
    drawn = jnp.clip(jax.random.normal(jax.random.fold_in(key, 23), (SEQS, SEQ, H * HD), jnp.float32), -4.0, 4.0)
    return drawn.astype(jnp.bfloat16)


def draw_chosen(key, part):
    blocks = jnp.arange(NBLK, dtype=jnp.int32)
    holder = blocks // BPD
    within = blocks % BPD
    query_dev = blocks // BPD
    query_in = blocks % BPD
    jitter = jax.random.randint(jax.random.fold_in(key, 3), (SEQS, N_KV, KVH, NBLK), 0, 1024)
    ranking = jitter * BPD + within
    ranking = jnp.where(blocks == 0, 1024 * BPD + 1, ranking)
    grouped = ranking.reshape(SEQS, N_KV, KVH, N_KV, BPD)
    order_rank = jnp.sum((grouped[..., None, :] > grouped[..., :, None]).astype(jnp.int32), axis=-1)
    usable = (order_rank < MOST).reshape(SEQS, N_KV, KVH, NBLK)
    usable_q = usable[:, query_dev]
    earlier = (holder[None, :] < query_dev[:, None])[None, :, None, :]
    own_ok = (holder[None, :] == query_dev[:, None]) & (within[None, :] <= query_in[:, None])
    forced = (own_ok | (blocks == 0)[None, :])[None, :, None, :]
    future = (blocks[None, :] > blocks[:, None])[None, :, None, :]
    levels = jnp.where(forced, 3, jnp.where(earlier & usable_q, 2, jnp.where(future, 1, 0)))
    pick_noise = jax.random.randint(jax.random.fold_in(key, 5), (SEQS, NBLK, KVH, NBLK), 0, 512)
    distance = query_dev[:, None] - holder[None, :]
    closeness = jnp.clip(512 - 64 * distance, 0, 1023)
    skewed = pick_noise + closeness[None, :, None, :]
    nearness = 1023 - jnp.minimum(jnp.abs(blocks[None, :] - blocks[:, None]), 1023)
    secondary = jnp.where(levels == 1, nearness[None, :, None, :], skewed)
    priority = levels * 2 ** 22 + secondary * NBLK + blocks[None, None, None, :]
    values_top, picked = lax.top_k(priority.astype(jnp.int32), TOPK)
    return picked.astype(jnp.int32)


def level_of(own_key, shape, shards, smallest, top_value):
    loudness = 1.0
    for axis_at, shards_of in shards:
        heights = jax.random.uniform(jax.random.fold_in(jax.random.fold_in(own_key, 6), axis_at), (shards_of,), jnp.float32, smallest / len(shards), top_value / len(shards))
        loudness = loudness * jnp.repeat(jnp.exp(heights), shape[axis_at] // shards_of).reshape((-1,) + (1,) * (len(shape) - 1 - axis_at))
    return loudness


def centred(key, shape, deviation, bound, shards=(), held_as=jnp.bfloat16):
    result = jax.random.normal(key, shape, jnp.float32) * deviation
    if len(shards) > 0:
        result = level_of(key, shape, shards, -0.22, 0.18) * result
    return jnp.clip(result, min=-bound, max=bound).astype(held_as)


def setup_inputs(seed: int = 0) -> dict:
    key_list = jax.random.split(jax.random.key(seed), 8)
    return {
        "queries": draw_queries(jax.random.fold_in(key_list[7], 71), 0),
        "key_states": draw_key_states(jax.random.fold_in(key_list[7], 71), 0),
        "value_states": centred(key_list[2], (SEQS, SEQ, KVH * HD), 1.0, 6.0, ((1, 8), (2, 4))),
        "cotangent": centred(key_list[3], (SEQS, SEQ, H * HD), 1.0, 6.0, ((1, 8), (2, 4))),
        "gate_logits": centred(key_list[4], (SEQS, SEQ, H), 1.5, 6.0, ((1, 8), (2, 4)), jnp.float32),
        "layer_input": centred(key_list[5], (SEQS, SEQ, D), 1.0, 6.0, ((1, 32),)),
        "chosen": draw_chosen(jax.random.fold_in(key_list[7], 71), 0),
    }


def reference(queries, key_states, value_states, cotangent, gate_logits, layer_input, chosen):
    seq_count, seq_len, row_width = queries.shape
    per_group = H // KVH
    total_blocks = seq_len // BLK
    score_scale = HD ** -0.5
    key_blocks = key_states.reshape(seq_count, total_blocks, BLK, KVH, HD)
    value_blocks = value_states.reshape(seq_count, total_blocks, BLK, KVH, HD)
    query_blocks = queries.reshape(seq_count, total_blocks, BLK, KVH, per_group, HD)
    grad_blocks = cotangent.reshape(seq_count, total_blocks, BLK, KVH, per_group, HD)
    gate_values = jax.nn.sigmoid(gate_logits.astype(jnp.float32)).reshape(seq_count, total_blocks, BLK, KVH, per_group)
    group_index = jnp.arange(KVH, dtype=jnp.int32)[:, None]
    offsets = jnp.arange(BLK, dtype=jnp.int32)

    def advance(totals, position):
        key_acc, value_acc = totals
        seq_index = position // total_blocks
        block_index = position % total_blocks
        picked = chosen[seq_index, block_index]
        picked_keys = key_blocks[seq_index][picked, :, group_index].astype(jnp.float32)
        picked_values = value_blocks[seq_index][picked, :, group_index].astype(jnp.float32)
        query_rows = query_blocks[seq_index, block_index].astype(jnp.float32)
        scores = jnp.einsum("qgpd,gknd->gpqkn", query_rows, picked_keys) * score_scale
        query_pos = block_index * BLK + offsets
        key_pos = picked[:, :, None] * BLK + offsets
        allowed = key_pos[:, None, None, :, :] <= query_pos[None, None, :, None, None]
        scores = jnp.where(allowed, scores, -jnp.inf)
        row_max = jnp.max(scores, axis=(3, 4), keepdims=True)
        exp_terms = jnp.exp(scores - row_max)
        weights = exp_terms / jnp.sum(exp_terms, axis=(3, 4), keepdims=True)
        weights_bf = weights.astype(jnp.bfloat16).astype(jnp.float32)
        branch_out = jnp.einsum("gpqkn,gknd->qgpd", weights_bf, picked_values)
        branch_grad = (gate_values[seq_index, block_index][..., None] * grad_blocks[seq_index, block_index].astype(jnp.float32)).astype(jnp.bfloat16).astype(jnp.float32)
        row_dot = jnp.sum(branch_grad * branch_out, axis=3)
        weight_grad = jnp.einsum("qgpd,gknd->gpqkn", branch_grad, picked_values)
        score_grad = (weights * (weight_grad - jnp.transpose(row_dot, (1, 2, 0))[..., None, None]) * score_scale).astype(jnp.bfloat16).astype(jnp.float32)
        query_grad = jnp.einsum("gpqkn,gknd->qgpd", score_grad, picked_keys).astype(jnp.bfloat16)
        pick_key = jnp.einsum("gpqkn,qgpd->gknd", score_grad, query_rows)
        pick_value = jnp.einsum("gpqkn,qgpd->gknd", weights_bf, branch_grad)
        key_acc = key_acc.at[seq_index, picked, :, group_index].add(pick_key)
        value_acc = value_acc.at[seq_index, picked, :, group_index].add(pick_value)
        return (key_acc, value_acc), query_grad

    empty = jnp.zeros((seq_count, total_blocks, BLK, KVH, HD), jnp.float32)
    (key_acc, value_acc), query_parts = lax.scan(advance, (empty, empty), jnp.arange(seq_count * total_blocks, dtype=jnp.int32))
    query_grad = query_parts.reshape(seq_count, seq_len, H * HD)
    key_grad = key_acc.reshape(seq_count, seq_len, KVH * HD).astype(jnp.bfloat16)
    value_grad = value_acc.reshape(seq_count, seq_len, KVH * HD).astype(jnp.bfloat16)
    value_weight_grad = jnp.einsum("std,ste->de", layer_input.astype(jnp.float32), value_grad.astype(jnp.float32))
    return query_grad, key_grad, value_grad, value_weight_grad
```

```python
import functools
import math

import jax
import jax.numpy as jnp
from jax import lax
from jax.experimental import pallas as pl
from jax.experimental.pallas import tpu as pltpu
from jax.sharding import PartitionSpec as P

BLK = 64
MOST = 2
LABEL_ROWS = 16
LOG2E = math.log2(math.e)
BF = jnp.bfloat16
F32 = jnp.float32
VMEM = pltpu.VMEM
SMEM = pltpu.SMEM
BIG_VMEM = pltpu.CompilerParams(vmem_limit_bytes=56 * 1024 * 1024)


def vspec():
    return pl.BlockSpec(memory_space=VMEM)


def sspec():
    return pl.BlockSpec(memory_space=SMEM)


def prep_kernel(heads, hd, scale, q_ref, g_ref, gate_ref, r_ref):
    width = 2 * hd
    rows = heads * BLK
    low = lax.broadcasted_iota(jnp.int32, (BLK, width), 1) < hd

    def step(i, carry):
        at = pl.ds(pl.multiple_of(i * BLK, BLK), BLK)
        gates = jax.nn.sigmoid(gate_ref[at, :])
        for pair in range(heads // 2):
            q = q_ref[at, pair * width : (pair + 1) * width].astype(F32) * scale
            g = g_ref[at, pair * width : (pair + 1) * width].astype(F32)
            gv = jnp.where(low, gates[:, 2 * pair : 2 * pair + 1], gates[:, 2 * pair + 1 : 2 * pair + 2])
            g = g * gv
            qr = pltpu.roll(q, hd, 1)
            gr = pltpu.roll(g, hd, 1)
            zero = jnp.zeros_like(q)
            base = 2 * pair * BLK
            r_ref[i, base : base + BLK, :] = jnp.where(low, q, zero).astype(BF)
            r_ref[i, base + BLK : base + 2 * BLK, :] = jnp.where(low, qr, zero).astype(BF)
            r_ref[i, rows + base : rows + base + BLK, :] = jnp.where(low, zero, gr).astype(BF)
            r_ref[i, rows + base + BLK : rows + base + 2 * BLK, :] = jnp.where(low, zero, g).astype(BF)
        return carry

    lax.fori_loop(0, q_ref.shape[0] // BLK, step, 0)


def pack_kernel(seqs, bpd, shifts, *refs):
    labels = refs[:shifts]
    pair_ref = refs[shifts]
    outs = refs[shifts + 1 :]
    for d in range(shifts):
        for s in range(seqs):
            for yh in range(2):
                for m in range(MOST):
                    slot = (s * 2 + yh) * MOST + m
                    lab = labels[d][d * seqs * 2 * MOST + slot]
                    src = pl.multiple_of(((yh * seqs + s) * bpd + lab) * BLK, BLK)
                    outs[d][slot * BLK : (slot + 1) * BLK, :] = pair_ref[pl.ds(src, BLK), :]


def attend_kernel(
    nblk, bpd, heads, hd, picks, shifts, zshifts, scale, kv_loc, acc_loc, labs, r_ref, pair_ref, *refs
):
    zmsgs = refs[:zshifts]
    dq_ref, own_ref = refs[zshifts : zshifts + 2]
    outs = refs[zshifts + 2 : zshifts + 2 + shifts]
    kv_all, kv_pick, s_buf, p_buf, x_buf, acc, dq_buf = refs[zshifts + 2 + shifts :]
    rows = heads * BLK
    width = 2 * hd
    seqs = nblk // bpd
    slots = seqs * MOST
    dummy = nblk + shifts * slots
    chunk = 4 * BLK
    keys = picks * BLK

    pair_rows = pair_ref.shape[0]
    kv_all[0:pair_rows, :] = pair_ref[...]
    for d in range(zshifts):
        n = zmsgs[d].shape[0]
        kv_all[pair_rows + d * n : pair_rows + (d + 1) * n, :] = zmsgs[d][...]
    acc[...] = jnp.zeros_like(acc)
    kpos = lax.broadcasted_iota(jnp.int32, (BLK, rows), 0)
    qpos = lax.broadcasted_iota(jnp.int32, (BLK, rows), 1) % BLK
    diag = kpos <= qpos

    def fold(x, op):
        out = x[0:8, :]
        for i in range(1, x.shape[0] // 8):
            out = op(out, x[i * 8 : (i + 1) * 8, :])
        return out

    def step(i, carry):
        base = i * picks
        for j in range(picks):
            src = pl.multiple_of(kv_loc[base + j] * BLK, BLK)
            kv_pick[j * BLK : (j + 1) * BLK, :] = kv_all[pl.ds(src, BLK), :]
        r = r_ref[i]
        top = jnp.full((8, rows), -jnp.inf, F32)
        for c in range(keys // chunk):
            both = lax.dot_general(
                kv_pick[c * chunk : (c + 1) * chunk, :], r, (((1,), (1,)), ((), ())), preferred_element_type=F32
            )
            p_buf[c * chunk : (c + 1) * chunk, :] = both[:, rows:]
            for j in range(4):
                pick = c * 4 + j
                s = both[j * BLK : (j + 1) * BLK, :rows] * LOG2E
                if pick == 0:
                    s = jnp.where(diag, s, -jnp.inf)
                else:
                    bias = jnp.where(acc_loc[base + pick] == dummy, -jnp.inf, 0.0).astype(F32)
                    s = s + bias
                s_buf[pick * BLK : (pick + 1) * BLK, :] = s
                top = jnp.maximum(top, fold(s, jnp.maximum))
        top = jnp.max(top, axis=0, keepdims=True)
        total = jnp.zeros((8, rows), F32)
        for j in range(picks):
            e = jnp.exp2(s_buf[j * BLK : (j + 1) * BLK, :] - top)
            total = total + fold(e, jnp.add)
        shift = top + jnp.log2(jnp.sum(total, axis=0, keepdims=True))
        dot = jnp.zeros((8, rows), F32)
        for j in range(picks):
            at = slice(j * BLK, (j + 1) * BLK)
            w = jnp.exp2(s_buf[at, :] - shift)
            wb = w.astype(BF)
            s_buf[at, :] = w
            x_buf[at, rows:] = wb
            dot = dot + fold(wb.astype(F32) * p_buf[at, :], jnp.add)
        dot = jnp.sum(dot, axis=0, keepdims=True)
        dqt = jnp.zeros((width, rows), F32)
        for c in range(keys // chunk):
            for j in range(4):
                at = slice((c * 4 + j) * BLK, (c * 4 + j + 1) * BLK)
                x_buf[at, :rows] = (s_buf[at, :] * (p_buf[at, :] - dot)).astype(BF)
            at = slice(c * chunk, (c + 1) * chunk)
            x = x_buf[at, :]
            grads = lax.dot_general(x, r, (((1,), (0,)), ((), ())), preferred_element_type=F32)
            for j in range(4):
                dst = pl.multiple_of(acc_loc[base + c * 4 + j] * BLK, BLK)
                acc[pl.ds(dst, BLK), :] += grads[j * BLK : (j + 1) * BLK, :]
            dqt = dqt + lax.dot_general(
                kv_pick[at, :], x[:, :rows], (((0,), (0,)), ((), ())), preferred_element_type=F32
            )
        dq_buf[...] = dqt[:hd, :] * scale
        row_at = pl.ds(pl.multiple_of(i * BLK, BLK), BLK)
        for pair in range(heads // 2):
            two = jnp.concatenate(
                [dq_buf[:, 2 * pair * BLK : (2 * pair + 1) * BLK], dq_buf[:, (2 * pair + 1) * BLK : (2 * pair + 2) * BLK]],
                axis=0,
            )
            dq_ref[row_at, pair * width : (pair + 1) * width] = two.T.astype(BF)
        return carry

    lax.fori_loop(0, nblk, step, 0)
    own_ref[...] = acc[0 : nblk * BLK, :]
    for d in range(shifts):
        lo = (nblk + d * slots) * BLK
        outs[d][0 : slots * BLK, :] = acc[lo : lo + slots * BLK, :].astype(BF)
        lane = lax.broadcasted_iota(jnp.int32, (LABEL_ROWS, width), 0)
        mark = jnp.zeros((LABEL_ROWS, width), F32)
        for k in range(slots):
            mark = jnp.where(lane == k, labs[d * slots + k].astype(F32), mark)
        outs[d][slots * BLK : slots * BLK + LABEL_ROWS, :] = mark.astype(BF)


def combine_kernel(seqs, bpd, hd, shifts, parts, quarter, own_ref, *refs):
    msgs = refs[:shifts]
    pieces = refs[shifts : shifts + parts]
    kg_ref, vg_ref, out_ref, total, vbuf = refs[shifts + parts :]
    slots = seqs * MOST
    total[...] = own_ref[...]
    width = 2 * hd
    for d in range(shifts):
        marks = msgs[d][slots * BLK : slots * BLK + LABEL_ROWS, :].astype(F32)
        for s in range(seqs):
            for m in range(MOST):
                k = s * MOST + m
                val = msgs[d][k * BLK : (k + 1) * BLK, :].astype(F32)
                mark = marks[k : k + 1, :]
                for b in range(bpd):
                    at = slice((s * bpd + b) * BLK, (s * bpd + b + 1) * BLK)
                    total[at, :] = total[at, :] + jnp.where(mark == float(b), val, 0.0)
    tok = bpd * BLK
    kg_ref[...] = total[:, :hd].astype(BF)
    vg = total[:, hd:].astype(BF)
    vg_ref[...] = vg
    vbuf[...] = vg
    span = tok // parts
    acc = None
    for j in range(parts):
        who = jnp.bitwise_xor(quarter[0], j)
        for s in range(seqs):
            lo = pl.multiple_of(s * tok + who * span, 16)
            v = vbuf[pl.ds(lo, span), :]
            one = lax.dot_general(
                v, pieces[j][s], (((0,), (0,)), ((), ())), preferred_element_type=F32
            )
            acc = one if acc is None else acc + one
    lanes = out_ref.shape[2]
    for i in range(out_ref.shape[0]):
        out_ref[i] = acc[:, i * lanes : (i + 1) * lanes].astype(BF)


def final_kernel(n, parts, in_ref, out_ref):
    for t in range(parts):
        acc = in_ref[t].astype(F32)
        for k in range(1, n):
            acc = acc + in_ref[k * parts + t].astype(F32)
        if t % 2 == 0:
            held = acc
        else:
            both = jnp.concatenate([held, acc], axis=0)
            w = both.shape[0]
            out_ref[:, (t // 2) * w : (t // 2 + 1) * w] = both.T


def on_device(queries, key_states, value_states, cotangent, gate_logits, layer_input, chosen):
    seqs, tok, row_width = queries.shape
    hd = key_states.shape[2]
    heads = row_width // hd
    bpd = tok // BLK
    picks = chosen.shape[3]
    n = lax.axis_size("kv")
    parts = lax.axis_size("tp")
    own = lax.axis_index("kv").astype(jnp.int32)
    t_own = lax.axis_index("tp").astype(jnp.int32)
    scale = hd ** (-0.5)
    assert math.log2(scale).is_integer() and n % 2 == 0
    nblk = seqs * bpd
    slots = seqs * MOST
    shifts = n - 1
    zshifts = n // 2 - 1
    width = 2 * hd

    perm = lambda x, axis, pairs: lax.ppermute(x, axis, pairs)
    tp_xor = lambda j: [(i, i ^ j) for i in range(parts)]
    piece2 = perm(layer_input, "tp", tp_xor(2))
    piece1 = perm(layer_input, "tp", tp_xor(1))
    piece3 = perm(piece2, "tp", tp_xor(1))
    pieces = [layer_input, piece1, piece2, piece3]

    ids = chosen[:, :, 0, :]
    flat = ids.reshape(seqs, bpd * picks)
    holder = flat // bpd
    within = flat % bpd

    dz = jnp.arange(1, zshifts + 1, dtype=jnp.int32)[:, None, None, None]
    yh = jnp.arange(2, dtype=jnp.int32)[None, None, :, None]
    target = 2 * (own // 2 - dz) + yh
    hit = holder[None, :, None, :] == target
    low = jnp.min(jnp.where(hit, within[None, :, None, :], bpd - 1), axis=-1)
    high = jnp.max(jnp.where(hit, within[None, :, None, :], 0), axis=-1)
    ask = jnp.stack([low, high], axis=-1).reshape(zshifts * seqs * 2 * MOST)
    asked = [
        perm(ask, "kv", [(k, k - 2 * d) for k in range(2 * d, n)]) for d in range(1, zshifts + 1)
    ]

    kv = jnp.concatenate([key_states, value_states], axis=-1).reshape(nblk * BLK, width)
    partner = perm(kv, "kv", [(k, k ^ 1) for k in range(n)])
    even = own % 2 == 0
    pair = jnp.where(even, jnp.concatenate([kv, partner]), jnp.concatenate([partner, kv]))

    zrows = slots * 2 * BLK
    packed = pl.pallas_call(
        functools.partial(pack_kernel, seqs, bpd, zshifts),
        out_shape=[jax.ShapeDtypeStruct((zrows, width), BF)] * zshifts,
        in_specs=[sspec()] * zshifts + [vspec()],
        out_specs=[vspec()] * zshifts,
        name="pack",
    )(*asked, pair)
    zmsgs = [
        perm(packed[d - 1], "kv", [(k, k + 2 * d) for k in range(n - 2 * d)]) for d in range(1, zshifts + 1)
    ]

    r = pl.pallas_call(
        functools.partial(prep_kernel, heads, hd, scale),
        out_shape=jax.ShapeDtypeStruct((nblk, 2 * heads * BLK, width), BF),
        in_specs=[vspec()] * 3,
        out_specs=vspec(),
        name="prep",
    )(
        queries.reshape(seqs * tok, row_width),
        cotangent.reshape(seqs * tok, row_width),
        gate_logits.reshape(seqs * tok, heads),
    )

    block = own * bpd + jnp.arange(bpd, dtype=jnp.int32)[None, :, None]
    first = ids[:, :, :1]
    at0 = lax.broadcasted_iota(jnp.int32, ids.shape, 2) == 0
    order = jnp.where(at0, block, jnp.where(ids == block, first, ids))
    h_of = order // bpd
    w_of = order % bpd
    low_of = jnp.min(
        jnp.where(h_of[..., None] == holder[:, None, None, :], within[:, None, None, :], bpd), axis=-1
    )
    slot = (w_of != low_of).astype(jnp.int32)
    seq = jnp.arange(seqs, dtype=jnp.int32)[:, None, None]
    in_pair = (h_of // 2) == (own // 2)
    z_at = 2 * nblk + ((own // 2 - h_of // 2 - 1) * seqs + seq) * 2 * MOST + (h_of % 2) * MOST + slot
    pair_at = ((h_of % 2) * seqs + seq) * bpd + w_of
    future = order > block
    kv_loc = jnp.where(future, 0, jnp.where(in_pair, pair_at, z_at)).reshape(-1)
    dummy = nblk + shifts * slots
    remote_at = nblk + ((own - h_of - 1) * seqs + seq) * MOST + slot
    acc_loc = jnp.where(future, dummy, jnp.where(h_of == own, seq * bpd + w_of, remote_at)).reshape(-1)
    back = own - jnp.arange(1, n, dtype=jnp.int32)[:, None, None]
    hit = holder[None] == back
    low = jnp.min(jnp.where(hit, within[None], bpd - 1), axis=-1)
    high = jnp.max(jnp.where(hit, within[None], 0), axis=-1)
    labs = jnp.stack([low, high], axis=-1).reshape(shifts * slots)

    keys = picks * BLK
    rows = heads * BLK
    mrows = slots * BLK + LABEL_ROWS
    attended = pl.pallas_call(
        functools.partial(attend_kernel, nblk, bpd, heads, hd, picks, shifts, zshifts, scale),
        out_shape=[
            jax.ShapeDtypeStruct((seqs * tok, row_width), BF),
            jax.ShapeDtypeStruct((nblk * BLK, width), F32),
        ]
        + [jax.ShapeDtypeStruct((mrows, width), BF)] * shifts,
        in_specs=[sspec()] * 3 + [vspec()] * (2 + zshifts),
        out_specs=[vspec()] * (2 + shifts),
        scratch_shapes=[
            VMEM((2 * nblk * BLK + zshifts * zrows, width), BF),
            VMEM((keys, width), BF),
            VMEM((keys, rows), F32),
            VMEM((keys, rows), F32),
            VMEM((keys, 2 * rows), BF),
            VMEM(((dummy + 1) * BLK, width), F32),
            VMEM((hd, rows), F32),
        ],
        compiler_params=BIG_VMEM,
        name="attend",
    )(kv_loc, acc_loc, labs, r, pair, *zmsgs)
    query_grad = attended[0].reshape(seqs, tok, row_width)
    own_sum = attended[1]
    arrived = [
        perm(attended[1 + d], "kv", [(k, k - d) for k in range(d, n)]) for d in range(1, n)
    ]

    ranks = n * parts
    depth = layer_input.shape[2]
    share = depth // ranks
    kg, vg, partial = pl.pallas_call(
        functools.partial(combine_kernel, seqs, bpd, hd, shifts, parts),
        out_shape=[
            jax.ShapeDtypeStruct((seqs * tok, hd), BF),
            jax.ShapeDtypeStruct((seqs * tok, hd), BF),
            jax.ShapeDtypeStruct((ranks * share // 128, hd, 128), BF),
        ],
        in_specs=[sspec()] + [vspec()] * (1 + shifts + parts),
        out_specs=[vspec()] * 3,
        scratch_shapes=[VMEM((nblk * BLK, width), F32), VMEM((seqs * tok, hd), BF)],
        compiler_params=BIG_VMEM,
        name="combine",
    )(t_own.reshape(1), own_sum, *arrived, *pieces)
    key_grad = kg.reshape(seqs, tok, hd)
    value_grad = vg.reshape(seqs, tok, hd)
    if share != 128:
        partial = partial.transpose(1, 0, 2).reshape(hd, ranks, share).transpose(1, 0, 2)
    swapped = lax.all_to_all(partial, ("kv", "tp"), split_axis=0, concat_axis=0, tiled=True)
    value_weight_grad = pl.pallas_call(
        functools.partial(final_kernel, n, parts),
        out_shape=jax.ShapeDtypeStruct((share, parts * hd), F32),
        in_specs=[vspec()],
        out_specs=vspec(),
        name="final",
    )(swapped)
    return query_grad, key_grad, value_grad, value_weight_grad


def solution(mesh):
    in_specs = (
        P(None, "kv", "tp"),
        P(None, "kv", "tp"),
        P(None, "kv", "tp"),
        P(None, "kv", "tp"),
        P(None, "kv", "tp"),
        P(None, ("kv", "tp"), None),
        P(None, "kv", "tp", None),
    )
    out_specs = (
        P(None, "kv", "tp"),
        P(None, "kv", "tp"),
        P(None, "kv", "tp"),
        P(("kv", "tp"), None),
    )
    return jax.shard_map(
        on_device, mesh=mesh, in_specs=in_specs, out_specs=out_specs, check_vma=False
    )
```

```python
import functools
import math

import jax
import jax.numpy as jnp
from jax import lax
from jax.experimental import pallas as pl
from jax.experimental.pallas import tpu as pltpu
from jax.sharding import PartitionSpec as P

BLK = 64
MOST = 2
LABEL_ROWS = 16
LOG2E = math.log2(math.e)
BF = jnp.bfloat16
F32 = jnp.float32
VMEM = pltpu.VMEM
SMEM = pltpu.SMEM
BIG_VMEM = pltpu.CompilerParams(vmem_limit_bytes=56 * 1024 * 1024)


def vspec():
    return pl.BlockSpec(memory_space=VMEM)


def sspec():
    return pl.BlockSpec(memory_space=SMEM)


def prep_kernel(
    n, bpd, picks, heads, hd, scale, ids, table, own_ref, q_ref, g_ref, gate_ref, r_ref, kv_loc, acc_loc
):
    width = 2 * hd
    rows = heads * BLK
    low = lax.broadcasted_iota(jnp.int32, (BLK, width), 1) < hd

    def step(i, carry):
        at = pl.ds(pl.multiple_of(i * BLK, BLK), BLK)
        gates = jax.nn.sigmoid(gate_ref[at, :])
        for pair in range(heads // 2):
            q = q_ref[at, pair * width : (pair + 1) * width].astype(F32) * scale
            g = g_ref[at, pair * width : (pair + 1) * width].astype(F32)
            gv = jnp.where(low, gates[:, 2 * pair : 2 * pair + 1], gates[:, 2 * pair + 1 : 2 * pair + 2])
            g = g * gv
            qr = pltpu.roll(q, hd, 1)
            gr = pltpu.roll(g, hd, 1)
            zero = jnp.zeros_like(q)
            base = 2 * pair * BLK
            r_ref[i, base : base + BLK, :] = jnp.where(low, q, zero).astype(BF)
            r_ref[i, base + BLK : base + 2 * BLK, :] = jnp.where(low, qr, zero).astype(BF)
            r_ref[i, rows + base : rows + base + BLK, :] = jnp.where(low, zero, gr).astype(BF)
            r_ref[i, rows + base + BLK : rows + base + 2 * BLK, :] = jnp.where(low, zero, g).astype(BF)
        return carry

    nblk = q_ref.shape[0] // BLK
    lax.fori_loop(0, nblk, step, 0)

    seqs = nblk // bpd
    own = own_ref[0]
    dummy = nblk + (n - 1) * seqs * MOST
    named = ids[...]
    row = lax.broadcasted_iota(jnp.int32, named.shape, 0)
    start = lax.broadcasted_iota(jnp.int32, named.shape, 1) == 0
    s = jnp.zeros_like(row)
    for k in range(1, seqs):
        s = s + (row >= k * bpd).astype(jnp.int32)
    block = own * bpd + row - s * bpd
    c = jnp.where(start, block, jnp.where(named == block, named[:, 0:1], named))
    h = lax.shift_right_logical(c * -(-(1 << 20) // bpd), 20)
    w = c - h * bpd
    low = jnp.zeros_like(c)
    for k in range(n):
        here = jnp.full_like(c, table[k * seqs])
        for q in range(1, seqs):
            here = jnp.where(s == q, table[k * seqs + q], here)
        low = jnp.where(h == k, here, low)
    slot = (w != low).astype(jnp.int32)
    own_z = lax.shift_right_logical(own, 1)
    h_z = lax.shift_right_logical(h, 1)
    home = s * bpd + w
    far = 2 * nblk + (((own_z - h_z - 1) * seqs + s) * 2 + (h & 1)) * MOST + slot
    near = jnp.where(h == own, home, nblk + home)
    future = c > block
    kv_loc[...] = jnp.where(future, 0, jnp.where(h_z == own_z, near, far))
    remote = nblk + ((own - h - 1) * seqs + s) * MOST + slot
    acc_loc[...] = jnp.where(future, dummy, jnp.where(h == own, home, remote))


def pack_kernel(seqs, bpd, n, shifts, *refs):
    tables = refs[:shifts]
    own_ref, kv_ref, partner_ref = refs[shifts : shifts + 3]
    outs = refs[shifts + 3 : 2 * shifts + 3]
    both = refs[2 * shifts + 3]
    rows = kv_ref.shape[0]
    both[0:rows, :] = kv_ref[...]
    both[rows : 2 * rows, :] = partner_ref[...]
    own = own_ref[0]
    side = own & 1
    for d in range(shifts):
        for s in range(seqs):
            for yh in range(2):
                for m in range(MOST):
                    slot = (s * 2 + yh) * MOST + m
                    lab = tables[d][m * n * seqs + (own - side + yh) * seqs + s]
                    at = ((side ^ yh) * seqs + s) * bpd + lab
                    src = pl.multiple_of(at * BLK, BLK)
                    outs[d][slot * BLK : (slot + 1) * BLK, :] = both[pl.ds(src, BLK), :]


def attend_kernel(
    nblk, bpd, heads, hd, picks, shifts, zshifts, scale, kv_loc, acc_loc, table, own_at, r_ref, kv_ref, partner_ref, *refs
):
    zmsgs = refs[:zshifts]
    dq_ref, own_ref = refs[zshifts : zshifts + 2]
    outs = refs[zshifts + 2 : zshifts + 2 + shifts]
    kv_all, acc, dq_buf = refs[zshifts + 2 + shifts : zshifts + 5 + shifts]
    sets = refs[zshifts + 5 + shifts :]
    kv_picks, s_bufs, p_bufs, x_bufs = sets[0:2], sets[2:4], sets[4:6], sets[6:8]
    rows = heads * BLK
    width = 2 * hd
    seqs = nblk // bpd
    slots = seqs * MOST
    dummy = nblk + shifts * slots
    chunk = 4 * BLK
    keys = picks * BLK

    pair_rows = 2 * nblk * BLK
    kv_all[0 : nblk * BLK, :] = kv_ref[...]
    kv_all[nblk * BLK : pair_rows, :] = partner_ref[...]
    for d in range(zshifts):
        n = zmsgs[d].shape[0]
        kv_all[pair_rows + d * n : pair_rows + (d + 1) * n, :] = zmsgs[d][...]
    acc[...] = jnp.zeros_like(acc)
    x_bufs[1][...] = jnp.zeros_like(x_bufs[1])
    kv_picks[1][...] = jnp.zeros_like(kv_picks[1])
    kpos = lax.broadcasted_iota(jnp.int32, (BLK, rows), 0)
    qpos = lax.broadcasted_iota(jnp.int32, (BLK, rows), 1) % BLK
    diag = kpos <= qpos

    def fold(x, op):
        out = x[0:8, :]
        for i in range(1, x.shape[0] // 8):
            out = op(out, x[i * 8 : (i + 1) * 8, :])
        return out

    def score(i, side):
        kv_pick, s_buf, p_buf = kv_picks[side], s_bufs[side], p_bufs[side]
        for j in range(picks):
            src = pl.multiple_of(kv_loc[i, j] * BLK, BLK)
            kv_pick[j * BLK : (j + 1) * BLK, :] = kv_all[pl.ds(src, BLK), :]
        r = r_ref[i]
        for c in range(keys // chunk):
            both = lax.dot_general(
                kv_pick[c * chunk : (c + 1) * chunk, :], r, (((1,), (1,)), ((), ())), preferred_element_type=F32
            )
            p_buf[c * chunk : (c + 1) * chunk, :] = both[:, rows:]
            for j in range(4):
                pick = c * 4 + j
                s = both[j * BLK : (j + 1) * BLK, :rows] * LOG2E
                if pick == 0:
                    s = jnp.where(diag, s, -jnp.inf)
                else:
                    bias = jnp.where(acc_loc[i, pick] == dummy, -jnp.inf, 0.0).astype(F32)
                    s = s + bias
                s_buf[pick * BLK : (pick + 1) * BLK, :] = s

    def weigh(side):
        s_buf, p_buf, x_buf = s_bufs[side], p_bufs[side], x_bufs[side]
        top = jnp.full((8, rows), -jnp.inf, F32)
        for j in range(picks):
            top = jnp.maximum(top, fold(s_buf[j * BLK : (j + 1) * BLK, :], jnp.maximum))
        top = jnp.max(top, axis=0, keepdims=True)
        total = jnp.zeros((8, rows), F32)
        for j in range(picks):
            e = jnp.exp2(s_buf[j * BLK : (j + 1) * BLK, :] - top)
            total = total + fold(e, jnp.add)
        shift = top + jnp.log2(jnp.sum(total, axis=0, keepdims=True))
        dot = jnp.zeros((8, rows), F32)
        for j in range(picks):
            at = slice(j * BLK, (j + 1) * BLK)
            w = jnp.exp2(s_buf[at, :] - shift)
            wb = w.astype(BF)
            s_buf[at, :] = w
            x_buf[at, rows:] = wb
            dot = dot + fold(wb.astype(F32) * p_buf[at, :], jnp.add)
        dot = jnp.sum(dot, axis=0, keepdims=True)
        for j in range(picks):
            at = slice(j * BLK, (j + 1) * BLK)
            x_buf[at, :rows] = (s_buf[at, :] * (p_buf[at, :] - dot)).astype(BF)

    def spread(i, side):
        kv_pick, x_buf = kv_picks[side], x_bufs[side]
        r = r_ref[i]
        dqt = jnp.zeros((width, rows), F32)
        for c in range(keys // chunk):
            at = slice(c * chunk, (c + 1) * chunk)
            x = x_buf[at, :]
            grads = lax.dot_general(x, r, (((1,), (0,)), ((), ())), preferred_element_type=F32)
            for j in range(4):
                dst = pl.multiple_of(acc_loc[i, c * 4 + j] * BLK, BLK)
                acc[pl.ds(dst, BLK), :] += grads[j * BLK : (j + 1) * BLK, :]
            dqt = dqt + lax.dot_general(
                kv_pick[at, :], x[:, :rows], (((0,), (0,)), ((), ())), preferred_element_type=F32
            )
        dq_buf[...] = dqt[:hd, :] * scale
        row_at = pl.ds(pl.multiple_of(i * BLK, BLK), BLK)
        for pair in range(heads // 2):
            two = jnp.concatenate(
                [dq_buf[:, 2 * pair * BLK : (2 * pair + 1) * BLK], dq_buf[:, (2 * pair + 1) * BLK : (2 * pair + 2) * BLK]],
                axis=0,
            )
            dq_ref[row_at, pair * width : (pair + 1) * width] = two.T.astype(BF)

    score(0, 0)

    def step(t, carry):
        i = 2 * t
        spread(jnp.maximum(i - 1, 0), 1)
        weigh(0)
        score(i + 1, 1)
        spread(i, 0)
        weigh(1)
        score(jnp.minimum(i + 2, nblk - 1), 0)
        return carry

    lax.fori_loop(0, nblk // 2, step, 0)
    spread(nblk - 1, 1)
    own_ref[...] = acc[0 : nblk * BLK, :]
    for d in range(shifts):
        lo = (nblk + d * slots) * BLK
        outs[d][0 : slots * BLK, :] = acc[lo : lo + slots * BLK, :].astype(BF)
        lane = lax.broadcasted_iota(jnp.int32, (LABEL_ROWS, width), 0)
        mark = jnp.zeros((LABEL_ROWS, width), F32)
        for k in range(slots):
            h = jnp.maximum(own_at[0] - d - 1, 0)
            lab = table[(k % MOST) * (shifts + 1) * seqs + h * seqs + k // MOST]
            mark = jnp.where(lane == k, lab.astype(F32), mark)
        outs[d][slots * BLK : slots * BLK + LABEL_ROWS, :] = mark.astype(BF)


def combine_kernel(seqs, bpd, hd, shifts, parts, quarter, own_ref, *refs):
    msgs = refs[:shifts]
    pieces = refs[shifts : shifts + parts]
    kg_ref, vg_ref, out_ref, total, vbuf = refs[shifts + parts :]
    slots = seqs * MOST
    total[...] = own_ref[...]
    width = 2 * hd
    for d in range(shifts):
        marks = msgs[d][slots * BLK : slots * BLK + LABEL_ROWS, :].astype(F32)
        for s in range(seqs):
            for m in range(MOST):
                k = s * MOST + m
                val = msgs[d][k * BLK : (k + 1) * BLK, :].astype(F32)
                mark = marks[k : k + 1, :]
                for b in range(bpd):
                    at = slice((s * bpd + b) * BLK, (s * bpd + b + 1) * BLK)
                    total[at, :] = total[at, :] + jnp.where(mark == float(b), val, 0.0)
    tok = bpd * BLK
    kg_ref[...] = total[:, :hd].astype(BF)
    vg = total[:, hd:].astype(BF)
    vg_ref[...] = vg
    vbuf[...] = vg
    span = tok // parts
    turned = []
    for j in range(parts):
        who = jnp.bitwise_xor(quarter[0], j)
        v = [
            vbuf[pl.ds(pl.multiple_of(s * tok + who * span, 16), span), :].astype(F32)
            for s in range(seqs)
        ]
        turned.append(jnp.concatenate(v, axis=0).T.astype(BF))
    lanes = out_ref.shape[2]
    for i in range(out_ref.shape[0] // 2):
        acc = jnp.zeros((hd, 2 * lanes), F32)
        for j in range(parts):
            x = pieces[j][:, 2 * i * lanes : 2 * (i + 1) * lanes]
            acc = acc + jnp.dot(turned[j], x, preferred_element_type=F32)
        out_ref[2 * i] = acc[:, :lanes].astype(BF)
        out_ref[2 * i + 1] = acc[:, lanes:].astype(BF)


def final_kernel(n, parts, in_ref, out_ref):
    for t in range(parts):
        acc = in_ref[t].astype(F32)
        for k in range(1, n):
            acc = acc + in_ref[k * parts + t].astype(F32)
        if t % 2 == 0:
            held = acc
        else:
            both = jnp.concatenate([held, acc], axis=0)
            w = both.shape[0]
            out_ref[:, (t // 2) * w : (t // 2 + 1) * w] = both.T


def on_device(queries, key_states, value_states, cotangent, gate_logits, layer_input, chosen):
    seqs, tok, row_width = queries.shape
    hd = key_states.shape[2]
    heads = row_width // hd
    bpd = tok // BLK
    picks = chosen.shape[3]
    n = lax.axis_size("kv")
    parts = lax.axis_size("tp")
    own = lax.axis_index("kv").astype(jnp.int32)
    t_own = lax.axis_index("tp").astype(jnp.int32)
    scale = hd ** (-0.5)
    assert math.log2(scale).is_integer() and n % 2 == 0
    nblk = seqs * bpd
    slots = seqs * MOST
    shifts = n - 1
    zshifts = n // 2 - 1
    width = 2 * hd

    perm = lax.ppermute
    kv = jnp.concatenate([key_states, value_states], axis=-1).reshape(nblk * BLK, width)
    partner = perm(kv, "kv", [(k, k ^ 1) for k in range(n)])

    ids = chosen[:, :, 0, :]
    flat = ids.reshape(seqs, bpd * picks)
    holder = (flat // bpd)[None]
    within = (flat % bpd)[None]
    hit = holder == jnp.arange(n, dtype=jnp.int32)[:, None, None]
    low = jnp.min(jnp.where(hit, within, bpd - 1), axis=-1)
    high = jnp.max(jnp.where(hit, within, 0), axis=-1)
    table = jnp.stack([low, high]).reshape(MOST * n * seqs)
    own_at = own.reshape(1)
    asked = [
        perm(table, "kv", [(k, k - 2 * d) for k in range(2 * d, n)]) for d in range(1, zshifts + 1)
    ]

    tp_xor = lambda j: [(i, i ^ j) for i in range(parts)]
    mine = layer_input.reshape(seqs * layer_input.shape[1], layer_input.shape[2])
    held, _ = lax.optimization_barrier((mine, table))
    piece2 = perm(held, "tp", tp_xor(2))
    piece1 = perm(held, "tp", tp_xor(1))

    r, kv_loc, acc_loc = pl.pallas_call(
        functools.partial(prep_kernel, n, bpd, picks, heads, hd, scale),
        out_shape=[
            jax.ShapeDtypeStruct((nblk, 2 * heads * BLK, width), BF),
            jax.ShapeDtypeStruct((nblk, picks), jnp.int32),
            jax.ShapeDtypeStruct((nblk, picks), jnp.int32),
        ],
        in_specs=[vspec()] + [sspec()] * 2 + [vspec()] * 3,
        out_specs=[vspec()] * 3,
        name="prep",
    )(
        ids.reshape(nblk, picks),
        table,
        own_at,
        queries.reshape(seqs * tok, row_width),
        cotangent.reshape(seqs * tok, row_width),
        gate_logits.reshape(seqs * tok, heads),
    )

    zrows = slots * 2 * BLK
    packed = pl.pallas_call(
        functools.partial(pack_kernel, seqs, bpd, n, zshifts),
        out_shape=[jax.ShapeDtypeStruct((zrows, width), BF)] * zshifts,
        in_specs=[sspec()] * (zshifts + 1) + [vspec()] * 2,
        out_specs=[vspec()] * zshifts,
        scratch_shapes=[VMEM((2 * nblk * BLK, width), BF)],
        name="pack",
    )(*asked, own_at, kv, partner)
    zmsgs = [
        perm(packed[d - 1], "kv", [(k, k + 2 * d) for k in range(n - 2 * d)]) for d in range(1, zshifts + 1)
    ]
    dummy = nblk + shifts * slots

    keys = picks * BLK
    rows = heads * BLK
    mrows = slots * BLK + LABEL_ROWS
    attended = pl.pallas_call(
        functools.partial(attend_kernel, nblk, bpd, heads, hd, picks, shifts, zshifts, scale),
        out_shape=[
            jax.ShapeDtypeStruct((seqs * tok, row_width), BF),
            jax.ShapeDtypeStruct((nblk * BLK, width), F32),
        ]
        + [jax.ShapeDtypeStruct((mrows, width), BF)] * shifts,
        in_specs=[sspec()] * 4 + [vspec()] * (3 + zshifts),
        out_specs=[vspec()] * (2 + shifts),
        scratch_shapes=[
            VMEM((2 * nblk * BLK + zshifts * zrows, width), BF),
            VMEM(((dummy + 1) * BLK, width), F32),
            VMEM((hd, rows), F32),
        ]
        + [VMEM((keys, width), BF)] * 2
        + [VMEM((keys, rows), F32)] * 4
        + [VMEM((keys, 2 * rows), BF)] * 2,
        compiler_params=BIG_VMEM,
        name="attend",
    )(kv_loc, acc_loc, table, own_at, r, kv, partner, *zmsgs)
    query_grad = attended[0].reshape(seqs, tok, row_width)
    own_sum, piece2 = lax.optimization_barrier((attended[1], piece2))
    piece3 = perm(piece2, "tp", tp_xor(1))
    pieces = [mine, piece1, piece2, piece3]
    arrived = [
        perm(attended[1 + d], "kv", [(k, k - d) for k in range(d, n)]) for d in range(1, n)
    ]

    ranks = n * parts
    depth = layer_input.shape[2]
    share = depth // ranks
    kg, vg, partial = pl.pallas_call(
        functools.partial(combine_kernel, seqs, bpd, hd, shifts, parts),
        out_shape=[
            jax.ShapeDtypeStruct((seqs * tok, hd), BF),
            jax.ShapeDtypeStruct((seqs * tok, hd), BF),
            jax.ShapeDtypeStruct((ranks * share // 128, hd, 128), BF),
        ],
        in_specs=[sspec()] + [vspec()] * (1 + shifts + parts),
        out_specs=[vspec()] * 3,
        scratch_shapes=[VMEM((nblk * BLK, width), F32), VMEM((seqs * tok, hd), BF)],
        compiler_params=BIG_VMEM,
        name="combine",
    )(t_own.reshape(1), own_sum, *arrived, *pieces)
    key_grad = kg.reshape(seqs, tok, hd)
    value_grad = vg.reshape(seqs, tok, hd)
    if share != 128:
        partial = partial.transpose(1, 0, 2).reshape(hd, ranks, share).transpose(1, 0, 2)
    swapped = lax.all_to_all(partial, ("kv", "tp"), split_axis=0, concat_axis=0, tiled=True)
    value_weight_grad = pl.pallas_call(
        functools.partial(final_kernel, n, parts),
        out_shape=jax.ShapeDtypeStruct((share, parts * hd), F32),
        in_specs=[vspec()],
        out_specs=vspec(),
        name="final",
    )(swapped)
    return query_grad, key_grad, value_grad, value_weight_grad


def solution(mesh):
    in_specs = (
        P(None, "kv", "tp"),
        P(None, "kv", "tp"),
        P(None, "kv", "tp"),
        P(None, "kv", "tp"),
        P(None, "kv", "tp"),
        P(None, ("kv", "tp"), None),
        P(None, "kv", "tp", None),
    )
    out_specs = (
        P(None, "kv", "tp"),
        P(None, "kv", "tp"),
        P(None, "kv", "tp"),
        P(("kv", "tp"), None),
    )
    return jax.shard_map(
        on_device, mesh=mesh, in_specs=in_specs, out_specs=out_specs, check_vma=False
    )
```

```python
import functools
import math

import jax
import jax.numpy as jnp
from jax import lax
from jax.experimental import pallas as pl
from jax.experimental.pallas import tpu as pltpu
from jax.sharding import PartitionSpec as P


BLK = 64
MOST = 2
LABEL_ROWS = 16
CUTS = 4
LOG2E = math.log2(math.e)
KV = ("hi", "lo")
BF = jnp.bfloat16
F32 = jnp.float32
VMEM = pltpu.VMEM
SMEM = pltpu.SMEM
MIB = 1024 * 1024


def grant(mib):
    return pltpu.CompilerParams(vmem_limit_bytes=mib * MIB)


def vspec():
    return pl.BlockSpec(memory_space=VMEM)


def sspec():
    return pl.BlockSpec(memory_space=SMEM)


def prep_kernel(
    n, bpd, heads, hd, scale, ids, table, own_ref, q_ref, g_ref, gate_ref, r_ref, kv_loc, acc_loc
):
    width = 2 * hd
    rows = heads * BLK
    low = lax.broadcasted_iota(jnp.int32, (BLK, width), 1) < hd

    def step(i, carry):
        at = pl.ds(pl.multiple_of(i * BLK, BLK), BLK)
        gates = jax.nn.sigmoid(gate_ref[at, :])
        for pair in range(heads // 2):
            q = q_ref[at, pair * width : (pair + 1) * width].astype(F32) * scale
            g = g_ref[at, pair * width : (pair + 1) * width].astype(F32)
            gv = jnp.where(low, gates[:, 2 * pair : 2 * pair + 1], gates[:, 2 * pair + 1 : 2 * pair + 2])
            g = g * gv
            qr = pltpu.roll(q, hd, 1)
            gr = pltpu.roll(g, hd, 1)
            zero = jnp.zeros_like(q)
            base = 2 * pair * BLK
            r_ref[i, base : base + BLK, :] = jnp.where(low, q, zero).astype(BF)
            r_ref[i, base + BLK : base + 2 * BLK, :] = jnp.where(low, qr, zero).astype(BF)
            r_ref[i, rows + base : rows + base + BLK, :] = jnp.where(low, zero, gr).astype(BF)
            r_ref[i, rows + base + BLK : rows + base + 2 * BLK, :] = jnp.where(low, zero, g).astype(BF)
        return carry

    nblk = q_ref.shape[0] // BLK
    lax.fori_loop(0, nblk, step, 0)

    seqs = nblk // bpd
    own = own_ref[0]
    dummy = nblk + n * seqs * MOST
    named = ids[...]
    row = lax.broadcasted_iota(jnp.int32, named.shape, 0)
    start = lax.broadcasted_iota(jnp.int32, named.shape, 1) == 0
    s = jnp.zeros_like(row)
    for k in range(1, seqs):
        s = s + (row >= k * bpd).astype(jnp.int32)
    block = own * bpd + row - s * bpd
    c = jnp.where(start, block, jnp.where(named == block, named[:, 0:1], named))
    h = lax.shift_right_logical(c * -(-(1 << 20) // bpd), 20)
    w = c - h * bpd
    low = jnp.zeros_like(c)
    for k in range(n):
        here = jnp.full_like(c, table[k * seqs])
        for q in range(1, seqs):
            here = jnp.where(s == q, table[k * seqs + q], here)
        low = jnp.where(h == k, here, low)
    slot = (w != low).astype(jnp.int32)
    own_z = lax.shift_right_logical(own, 1)
    h_z = lax.shift_right_logical(h, 1)
    home = s * bpd + w
    far = 2 * nblk + (((own_z - h_z - 1) * seqs + s) * 2 + (h & 1)) * MOST + slot
    near = jnp.where(h == own, home, nblk + home)
    future = c > block
    kv_loc[...] = jnp.where(future, 0, jnp.where(h_z == own_z, near, far))
    remote = nblk + (h * seqs + s) * MOST + slot
    acc_loc[...] = jnp.where(future, dummy, jnp.where(h == own, home, remote))


def pack_kernel(seqs, bpd, n, shifts, *refs):
    tables = refs[:shifts]
    own_ref, kv_ref, partner_ref = refs[shifts : shifts + 3]
    outs = refs[shifts + 3 : 2 * shifts + 3]
    both = refs[2 * shifts + 3]
    rows = kv_ref.shape[0]
    both[0:rows, :] = kv_ref[...]
    both[rows : 2 * rows, :] = partner_ref[...]
    own = own_ref[0]
    side = own & 1
    for d in range(shifts):
        for s in range(seqs):
            for yh in range(2):
                for m in range(MOST):
                    slot = (s * 2 + yh) * MOST + m
                    lab = tables[d][m * n * seqs + (own - side + yh) * seqs + s]
                    at = ((side ^ yh) * seqs + s) * bpd + lab
                    src = pl.multiple_of(at * BLK, BLK)
                    outs[d][slot * BLK : (slot + 1) * BLK, :] = both[pl.ds(src, BLK), :]


def attend_kernel(
    n,
    nblk,
    bpd,
    heads,
    hd,
    picks,
    scale,
    kv_loc,
    acc_loc,
    table,
    r_ref,
    kv_ref,
    partner_ref,
    *refs,
):
    zshifts = n // 2 - 1
    far = refs[:zshifts]
    dq_ref, own_ref, out_ref, kv_all, acc, dq_buf = refs[zshifts : zshifts + 6]
    sets = refs[zshifts + 6 :]
    kv_picks, s_bufs, p_bufs, x_bufs = sets[0:2], sets[2:4], sets[4:6], sets[6:8]
    rows = heads * BLK
    width = 2 * hd
    seqs = nblk // bpd
    slots = seqs * MOST
    dummy = nblk + n * slots
    chunk = 4 * BLK
    keys = picks * BLK

    pair_rows = 2 * nblk * BLK
    kv_all[0 : nblk * BLK, :] = kv_ref[...]
    kv_all[nblk * BLK : pair_rows, :] = partner_ref[...]
    for d in range(zshifts):
        span = far[d].shape[0]
        kv_all[pair_rows + d * span : pair_rows + (d + 1) * span, :] = far[d][...]
    acc[...] = jnp.zeros_like(acc)
    x_bufs[1][...] = jnp.zeros_like(x_bufs[1])
    kv_picks[1][...] = jnp.zeros_like(kv_picks[1])
    kpos = lax.broadcasted_iota(jnp.int32, (BLK, rows), 0)
    qpos = lax.broadcasted_iota(jnp.int32, (BLK, rows), 1) % BLK
    diag = kpos <= qpos

    def fold(x, op):
        out = x[0:8, :]
        for i in range(1, x.shape[0] // 8):
            out = op(out, x[i * 8 : (i + 1) * 8, :])
        return out

    def gather(i, side):
        for j in range(picks):
            src = pl.multiple_of(kv_loc[i, j] * BLK, BLK)
            kv_picks[side][j * BLK : (j + 1) * BLK, :] = kv_all[pl.ds(src, BLK), :]

    def score(i, side):
        kv_pick, s_buf, p_buf = kv_picks[side], s_bufs[side], p_bufs[side]
        r = r_ref[i]
        for c in range(keys // chunk):
            both = lax.dot_general(
                kv_pick[c * chunk : (c + 1) * chunk, :], r, (((1,), (1,)), ((), ())), preferred_element_type=F32
            )
            p_buf[c * chunk : (c + 1) * chunk, :] = both[:, rows:]
            for j in range(4):
                pick = c * 4 + j
                s = both[j * BLK : (j + 1) * BLK, :rows] * LOG2E
                if pick == 0:
                    s = jnp.where(diag, s, -jnp.inf)
                else:
                    bias = jnp.where(acc_loc[i, pick] == dummy, -jnp.inf, 0.0).astype(F32)
                    s = s + bias
                s_buf[pick * BLK : (pick + 1) * BLK, :] = s
            yield

    def weigh(side):
        s_buf, p_buf, x_buf = s_bufs[side], p_bufs[side], x_bufs[side]
        top = jnp.full((8, rows), -jnp.inf, F32)
        for j in range(picks):
            top = jnp.maximum(top, fold(s_buf[j * BLK : (j + 1) * BLK, :], jnp.maximum))
            yield 1
        top = jnp.max(top, axis=0, keepdims=True)
        total = jnp.zeros((8, rows), F32)
        for j in range(picks):
            e = jnp.exp2(s_buf[j * BLK : (j + 1) * BLK, :] - top)
            total = total + fold(e, jnp.add)
            yield 3
        shift = top + jnp.log2(jnp.sum(total, axis=0, keepdims=True))
        dot = jnp.zeros((8, rows), F32)
        for j in range(picks):
            at = slice(j * BLK, (j + 1) * BLK)
            w = jnp.exp2(s_buf[at, :] - shift)
            wb = w.astype(BF)
            s_buf[at, :] = w
            x_buf[at, rows:] = wb
            dot = dot + fold(wb.astype(F32) * p_buf[at, :], jnp.add)
            yield 6
        dot = jnp.sum(dot, axis=0, keepdims=True)
        for j in range(picks):
            at = slice(j * BLK, (j + 1) * BLK)
            x_buf[at, :rows] = (s_buf[at, :] * (p_buf[at, :] - dot)).astype(BF)
            yield 3

    def spread(i, side):
        kv_pick, x_buf = kv_picks[side], x_bufs[side]
        r = r_ref[i]
        dqt = jnp.zeros((width, rows), F32)
        for c in range(keys // chunk):
            at = slice(c * chunk, (c + 1) * chunk)
            x = x_buf[at, :]
            grads = lax.dot_general(x, r, (((1,), (0,)), ((), ())), preferred_element_type=F32)
            for j in range(4):
                dst = pl.multiple_of(acc_loc[i, c * 4 + j] * BLK, BLK)
                acc[pl.ds(dst, BLK), :] += grads[j * BLK : (j + 1) * BLK, :]
            dqt = dqt + lax.dot_general(
                kv_pick[at, :], x[:, :rows], (((0,), (0,)), ((), ())), preferred_element_type=F32
            )
            yield
        dq_buf[...] = dqt[:hd, :] * scale
        row_at = pl.ds(pl.multiple_of(i * BLK, BLK), BLK)
        for pair in range(heads // 2):
            two = jnp.concatenate(
                [dq_buf[:, 2 * pair * BLK : (2 * pair + 1) * BLK], dq_buf[:, (2 * pair + 1) * BLK : (2 * pair + 2) * BLK]],
                axis=0,
            )
            dq_ref[row_at, pair * width : (pair + 1) * width] = two.T.astype(BF)
        yield

    def drain(steps):
        for _ in steps:
            pass

    def turn(i, side):
        other = 1 - side
        after = jnp.minimum(i + 1, nblk - 1)

        def matmuls():
            yield from spread(jnp.maximum(i - 1, 0), other)
            gather(after, other)
            yield from score(after, other)

        pending = matmuls()
        parts = 2 * (keys // chunk) + 1
        whole = 13 * picks
        done = taken = 0
        for units in weigh(side):
            done += units
            while taken < parts and done * parts >= (taken + 1) * whole * 0.9:
                next(pending)
                taken += 1
        drain(pending)

    gather(0, 0)
    drain(score(0, 0))

    def step(i, carry):
        @pl.when(i % 2 == 0)
        def _():
            turn(i, 0)

        @pl.when(i % 2 == 1)
        def _():
            turn(i, 1)

        return carry

    lax.fori_loop(0, nblk, step, 0)
    drain(spread(nblk - 1, 1))
    own_ref[...] = acc[0 : nblk * BLK, :]
    lane = lax.broadcasted_iota(jnp.int32, (LABEL_ROWS, width), 0)
    for h in range(n):
        lo = (nblk + h * slots) * BLK
        out_ref[h, 0 : slots * BLK, :] = acc[lo : lo + slots * BLK, :].astype(BF)
        mark = jnp.zeros((LABEL_ROWS, width), F32)
        for k in range(slots):
            lab = table[(k % MOST) * n * seqs + h * seqs + k // MOST]
            mark = jnp.where(lane == k, lab.astype(F32), mark)
        out_ref[h, slots * BLK : slots * BLK + LABEL_ROWS, :] = mark.astype(BF)


def combine_kernel(n, seqs, bpd, hd, parts, quarter, own_ref, msgs, *refs):
    sources = refs[:parts]
    kg_ref, vg_ref, out_ref, total, vbuf, pieces, sems = refs[parts:]
    cut = sources[0].shape[0] // CUTS
    copies = [
        pltpu.make_async_copy(
            sources[j].at[pl.ds(q * cut, cut)], pieces.at[j, pl.ds(q * cut, cut)], sems.at[j, q]
        )
        for q in range(CUTS)
        for j in range(parts)
    ]
    for copy in copies:
        copy.start()
    slots = seqs * MOST
    total[...] = own_ref[...]
    for d in range(n):
        marks = msgs[d, slots * BLK : slots * BLK + LABEL_ROWS, :].astype(F32)
        for s in range(seqs):
            for m in range(MOST):
                k = s * MOST + m
                val = msgs[d, k * BLK : (k + 1) * BLK, :].astype(F32)
                mark = marks[k : k + 1, :]
                for b in range(bpd):
                    at = slice((s * bpd + b) * BLK, (s * bpd + b + 1) * BLK)
                    total[at, :] = total[at, :] + jnp.where(mark == float(b), val, 0.0)
    tok = bpd * BLK
    kg_ref[...] = total[:, :hd].astype(BF)
    vg = total[:, hd:].astype(BF)
    vg_ref[...] = vg
    vbuf[...] = vg
    span = tok // parts
    turned = []
    for j in range(parts):
        who = jnp.bitwise_xor(quarter[0], j)
        v = [
            vbuf[pl.ds(pl.multiple_of(s * tok + who * span, 16), span), :].astype(F32)
            for s in range(seqs)
        ]
        turned.append(jnp.concatenate(v, axis=0).T.astype(BF))
    lanes = out_ref.shape[2]
    for copy in copies:
        copy.wait()
    for i in range(out_ref.shape[0] // 2):
        acc = jnp.zeros((hd, 2 * lanes), F32)
        for j in range(parts):
            x = pieces[j, :, 2 * i * lanes : 2 * (i + 1) * lanes]
            acc = acc + jnp.dot(turned[j], x, preferred_element_type=F32)
        out_ref[2 * i] = acc[:, :lanes].astype(BF)
        out_ref[2 * i + 1] = acc[:, lanes:].astype(BF)


def final_kernel(n, parts, in_ref, out_ref):
    for t in range(parts):
        acc = in_ref[t].astype(F32)
        for k in range(1, n):
            acc = acc + in_ref[k * parts + t].astype(F32)
        if t % 2 == 0:
            held = acc
        else:
            both = jnp.concatenate([held, acc], axis=0)
            w = both.shape[0]
            out_ref[:, (t // 2) * w : (t // 2 + 1) * w] = both.T


def on_device(queries, key_states, value_states, cotangent, gate_logits, layer_input, chosen):
    seqs, tok, row_width = queries.shape
    hd = key_states.shape[2]
    heads = row_width // hd
    bpd = tok // BLK
    picks = chosen.shape[3]
    pairs = lax.axis_size("hi")
    n = 2 * pairs
    parts = lax.axis_size("tp")
    own = lax.axis_index(KV).astype(jnp.int32)
    t_own = lax.axis_index("tp").astype(jnp.int32)
    scale = hd ** (-0.5)
    assert math.log2(scale).is_integer() and n % 2 == 0
    nblk = seqs * bpd
    slots = seqs * MOST
    zshifts = pairs - 1
    width = 2 * hd

    perm = lax.ppermute
    kv = jnp.concatenate([key_states, value_states], axis=-1).reshape(nblk * BLK, width)
    partner = perm(kv, "lo", [(0, 1), (1, 0)])

    kv, chosen = lax.optimization_barrier((kv, chosen))
    ids = chosen[:, :, 0, :]
    flat = ids.reshape(seqs, bpd * picks)
    holder = (flat // bpd)[None]
    within = (flat % bpd)[None]
    hit = holder == jnp.arange(n, dtype=jnp.int32)[:, None, None]
    low = jnp.min(jnp.where(hit, within, bpd - 1), axis=-1)
    high = jnp.max(jnp.where(hit, within, 0), axis=-1)
    table = jnp.stack([low, high]).reshape(MOST * n * seqs)
    own_at = own.reshape(1)
    asked = [
        perm(table, "hi", [(k, k - d) for k in range(d, pairs)]) for d in range(1, pairs)
    ]

    tp_xor = lambda j: [(i, i ^ j) for i in range(parts)]
    mine = layer_input.reshape(seqs * layer_input.shape[1], layer_input.shape[2])
    piece2 = perm(mine, "tp", tp_xor(2))
    piece1 = perm(mine, "tp", tp_xor(1))

    prepare = pl.pallas_call(
        functools.partial(prep_kernel, n, bpd, heads, hd, scale),
        out_shape=[
            jax.ShapeDtypeStruct((nblk, 2 * heads * BLK, width), BF),
            jax.ShapeDtypeStruct((nblk, picks), jnp.int32),
            jax.ShapeDtypeStruct((nblk, picks), jnp.int32),
        ],
        in_specs=[vspec()] + [sspec()] * 2 + [vspec()] * 3,
        out_specs=[vspec()] * 3,
        compiler_params=grant(3),
        name="prep",
    )
    r, kv_loc, acc_loc = prepare(
        ids.reshape(nblk, picks),
        table,
        own_at,
        queries.reshape(seqs * tok, row_width),
        cotangent.reshape(seqs * tok, row_width),
        gate_logits.reshape(seqs * tok, heads),
    )

    zrows = slots * 2 * BLK
    packed = pl.pallas_call(
        functools.partial(pack_kernel, seqs, bpd, n, zshifts),
        out_shape=[jax.ShapeDtypeStruct((zrows, width), BF)] * zshifts,
        in_specs=[sspec()] * (zshifts + 1) + [vspec()] * 2,
        out_specs=[vspec()] * zshifts,
        scratch_shapes=[VMEM((2 * nblk * BLK, width), BF)],
        compiler_params=grant(3),
        name="pack",
    )(*asked, own_at, kv, partner)
    far = [
        perm(packed[d - 1], "hi", [(k, k + d) for k in range(pairs - d)]) for d in range(1, pairs)
    ]
    dummy = nblk + n * slots

    keys = picks * BLK
    rows = heads * BLK
    mrows = slots * BLK + LABEL_ROWS
    attended = pl.pallas_call(
        functools.partial(attend_kernel, n, nblk, bpd, heads, hd, picks, scale),
        out_shape=[
            jax.ShapeDtypeStruct((seqs * tok, row_width), BF),
            jax.ShapeDtypeStruct((nblk * BLK, width), F32),
            jax.ShapeDtypeStruct((n, mrows, width), BF),
        ],
        in_specs=[sspec()] * 3 + [vspec()] * (3 + zshifts),
        out_specs=[vspec()] * 3,
        scratch_shapes=[
            VMEM((2 * nblk * BLK + zshifts * zrows, width), BF),
            VMEM(((dummy + 1) * BLK, width), F32),
            VMEM((hd, rows), F32),
        ]
        + [VMEM((keys, width), BF)] * 2
        + [VMEM((keys, rows), F32)] * 4
        + [VMEM((keys, 2 * rows), BF)] * 2,
        compiler_params=grant(14),
        name="attend",
    )(kv_loc, acc_loc, table, r, kv, partner, *far)
    query_grad = attended[0].reshape(seqs, tok, row_width)
    arrived = lax.all_to_all(attended[2], KV, split_axis=0, concat_axis=0, tiled=True)
    own_sum, piece2 = lax.optimization_barrier((attended[1], piece2))
    piece3 = perm(piece2, "tp", tp_xor(1))
    pieces = [mine, piece1, piece2, piece3]

    ranks = n * parts
    depth = layer_input.shape[2]
    share = depth // ranks
    kg, vg, partial = pl.pallas_call(
        functools.partial(combine_kernel, n, seqs, bpd, hd, parts),
        out_shape=[
            jax.ShapeDtypeStruct((seqs * tok, hd), BF),
            jax.ShapeDtypeStruct((seqs * tok, hd), BF),
            jax.ShapeDtypeStruct((ranks * share // 128, hd, 128), BF),
        ],
        in_specs=[sspec()] + [vspec()] * 2 + [pl.BlockSpec(memory_space=pl.ANY)] * parts,
        out_specs=[vspec()] * 3,
        scratch_shapes=[
            VMEM((nblk * BLK, width), F32),
            VMEM((seqs * tok, hd), BF),
            VMEM((parts,) + mine.shape, BF),
            pltpu.SemaphoreType.DMA((parts, CUTS)),
        ],
        compiler_params=grant(10),
        name="combine",
    )(t_own.reshape(1), own_sum, arrived, *pieces)
    key_grad = kg.reshape(seqs, tok, hd)
    value_grad = vg.reshape(seqs, tok, hd)
    if share != 128:
        partial = partial.transpose(1, 0, 2).reshape(hd, ranks, share).transpose(1, 0, 2)
    swapped = lax.all_to_all(partial, KV + ("tp",), split_axis=0, concat_axis=0, tiled=True)
    value_weight_grad = pl.pallas_call(
        functools.partial(final_kernel, n, parts),
        out_shape=jax.ShapeDtypeStruct((share, parts * hd), F32),
        in_specs=[vspec()],
        out_specs=vspec(),
        compiler_params=grant(2),
        name="final",
    )(swapped)
    return query_grad, key_grad, value_grad, value_weight_grad


def solution(mesh):
    count = mesh.shape["kv"]
    split = jax.sharding.Mesh(
        mesh.devices.reshape(count // 2, 2, mesh.shape["tp"]), ("hi", "lo", "tp")
    )
    in_specs = (
        P(None, KV, "tp"),
        P(None, KV, "tp"),
        P(None, KV, "tp"),
        P(None, KV, "tp"),
        P(None, KV, "tp"),
        P(None, KV + ("tp",), None),
        P(None, KV, "tp", None),
    )
    out_specs = (
        P(None, KV, "tp"),
        P(None, KV, "tp"),
        P(None, KV, "tp"),
        P(KV + ("tp",), None),
    )

    return jax.shard_map(
        on_device, mesh=split, in_specs=in_specs, out_specs=out_specs, check_vma=False
    )
```

```python
import functools
import math

import jax
import jax.numpy as jnp
from jax import lax
from jax.experimental import pallas as pl
from jax.experimental.pallas import tpu as pltpu
from jax.sharding import PartitionSpec as P


BLK = 64
MOST = 2
LABEL_ROWS = 16
CUTS = 4
LOG2E = math.log2(math.e)
KV = ("hi", "lo")
BF = jnp.bfloat16
F32 = jnp.float32
VMEM = pltpu.VMEM
SMEM = pltpu.SMEM
MIB = 1024 * 1024


def grant(mib):
    return pltpu.CompilerParams(vmem_limit_bytes=mib * MIB)


def vspec():
    return pl.BlockSpec(memory_space=VMEM)


def sspec():
    return pl.BlockSpec(memory_space=SMEM)


def front_kernel(n, seqs, bpd, ids_ref, key_ref, value_ref, kv_ref, table_ref):
    tok = key_ref.shape[2]
    for s in range(seqs):
        both = jnp.concatenate([key_ref[s], value_ref[s]], axis=0).astype(F32)
        kv_ref[s * tok : (s + 1) * tok, :] = both.T.astype(BF)
    lane = lax.broadcasted_iota(jnp.int32, table_ref.shape, 1)
    table = jnp.zeros(table_ref.shape, jnp.int32)
    for s in range(seqs):
        c = ids_ref[s, :, 0, :]
        h = lax.shift_right_logical(c * -(-(1 << 20) // bpd), 20)
        w = c - h * bpd
        for k in range(n):
            low = jnp.min(jnp.where(h == k, w, bpd - 1).astype(F32), keepdims=True)
            high = jnp.max(jnp.where(h == k, w, 0).astype(F32), keepdims=True)
            table = jnp.where(lane == k * seqs + s, low.astype(jnp.int32), table)
            table = jnp.where(lane == (n + k) * seqs + s, high.astype(jnp.int32), table)
    table_ref[...] = table


def prep_kernel(
    n,
    seqs,
    bpd,
    heads,
    hd,
    scale,
    table,
    own_ref,
    ids,
    gate_ref,
    q_ref,
    g_ref,
    r_ref,
    kv_loc,
    acc_loc,
    gate_buf,
):
    width = 2 * hd
    rows = heads * BLK
    tok = bpd * BLK
    for s in range(seqs):
        gate_buf[s * tok : (s + 1) * tok, :] = jax.nn.sigmoid(gate_ref[s]).T
    front = lax.broadcasted_iota(jnp.int32, (BLK, width), 1) < hd

    def step(i, carry):
        at = pl.ds(pl.multiple_of(i * BLK, BLK), BLK)
        gates = gate_buf[at, :]
        for pair in range(heads // 2):
            q = q_ref[at, pair * width : (pair + 1) * width].astype(F32) * scale
            g = g_ref[at, pair * width : (pair + 1) * width].astype(F32)
            gv = jnp.where(front, gates[:, 2 * pair : 2 * pair + 1], gates[:, 2 * pair + 1 : 2 * pair + 2])
            g = g * gv
            qr = pltpu.roll(q, hd, 1)
            gr = pltpu.roll(g, hd, 1)
            zero = jnp.zeros_like(q)
            base = 2 * pair * BLK
            r_ref[i, base : base + BLK, :] = jnp.where(front, q, zero).astype(BF)
            r_ref[i, base + BLK : base + 2 * BLK, :] = jnp.where(front, qr, zero).astype(BF)
            r_ref[i, rows + base : rows + base + BLK, :] = jnp.where(front, zero, gr).astype(BF)
            r_ref[i, rows + base + BLK : rows + base + 2 * BLK, :] = jnp.where(front, zero, g).astype(BF)
        return carry

    nblk = seqs * bpd
    own = own_ref[0]
    dummy = nblk + n * seqs * MOST
    named = jnp.concatenate([ids[s, :, 0, :] for s in range(seqs)], axis=0)
    row = lax.broadcasted_iota(jnp.int32, named.shape, 0)
    start = lax.broadcasted_iota(jnp.int32, named.shape, 1) == 0
    s = jnp.zeros_like(row)
    for k in range(1, seqs):
        s = s + (row >= k * bpd).astype(jnp.int32)
    block = own * bpd + row - s * bpd
    c = jnp.where(start, block, jnp.where(named == block, named[:, 0:1], named))
    h = lax.shift_right_logical(c * -(-(1 << 20) // bpd), 20)
    w = c - h * bpd
    low = jnp.zeros_like(c)
    for k in range(n):
        here = jnp.full_like(c, table[0, k * seqs])
        for q in range(1, seqs):
            here = jnp.where(s == q, table[0, k * seqs + q], here)
        low = jnp.where(h == k, here, low)
    slot = (w != low).astype(jnp.int32)
    own_z = lax.shift_right_logical(own, 1)
    h_z = lax.shift_right_logical(h, 1)
    home = s * bpd + w
    far = 2 * nblk + (((own_z - h_z - 1) * seqs + s) * 2 + (h & 1)) * MOST + slot
    near = jnp.where(h == own, home, nblk + home)
    future = c > block
    kv_loc[...] = jnp.where(future, 0, jnp.where(h_z == own_z, near, far))
    remote = nblk + (h * seqs + s) * MOST + slot
    acc_loc[...] = jnp.where(future, dummy, jnp.where(h == own, home, remote))

    lax.fori_loop(0, nblk, step, 0)


def pack_kernel(seqs, bpd, n, shifts, *refs):
    tables = refs[:shifts]
    own_ref, kv_ref, partner_ref = refs[shifts : shifts + 3]
    outs = refs[shifts + 3 : 2 * shifts + 3]
    both = refs[2 * shifts + 3]
    rows = kv_ref.shape[0]
    both[0:rows, :] = kv_ref[...]
    both[rows : 2 * rows, :] = partner_ref[...]
    own = own_ref[0]
    side = own & 1
    for d in range(shifts):
        for s in range(seqs):
            for yh in range(2):
                for m in range(MOST):
                    slot = (s * 2 + yh) * MOST + m
                    lab = tables[d][0, m * n * seqs + (own - side + yh) * seqs + s]
                    at = ((side ^ yh) * seqs + s) * bpd + lab
                    src = pl.multiple_of(at * BLK, BLK)
                    outs[d][slot * BLK : (slot + 1) * BLK, :] = both[pl.ds(src, BLK), :]


def attend_kernel(
    n,
    nblk,
    bpd,
    heads,
    hd,
    picks,
    scale,
    kv_loc,
    acc_loc,
    table,
    r_ref,
    kv_ref,
    partner_ref,
    *refs,
):
    zshifts = n // 2 - 1
    far = refs[:zshifts]
    dq_ref, own_ref, out_ref, kv_all, acc, dq_buf = refs[zshifts : zshifts + 6]
    sets = refs[zshifts + 6 :]
    kv_picks, s_bufs, p_bufs, x_bufs = sets[0:2], sets[2:4], sets[4:6], sets[6:8]
    rows = heads * BLK
    width = 2 * hd
    seqs = nblk // bpd
    slots = seqs * MOST
    dummy = nblk + n * slots
    chunk = 4 * BLK
    keys = picks * BLK

    pair_rows = 2 * nblk * BLK
    kv_all[0 : nblk * BLK, :] = kv_ref[...]
    kv_all[nblk * BLK : pair_rows, :] = partner_ref[...]
    for d in range(zshifts):
        span = far[d].shape[0]
        kv_all[pair_rows + d * span : pair_rows + (d + 1) * span, :] = far[d][...]
    acc[...] = jnp.zeros_like(acc)
    x_bufs[1][...] = jnp.zeros_like(x_bufs[1])
    kv_picks[1][...] = jnp.zeros_like(kv_picks[1])
    kpos = lax.broadcasted_iota(jnp.int32, (BLK, rows), 0)
    qpos = lax.broadcasted_iota(jnp.int32, (BLK, rows), 1) % BLK
    diag = kpos <= qpos

    def fold(x, op):
        out = x[0:8, :]
        for i in range(1, x.shape[0] // 8):
            out = op(out, x[i * 8 : (i + 1) * 8, :])
        return out

    def gather(i, side):
        for j in range(picks):
            src = pl.multiple_of(kv_loc[i, j] * BLK, BLK)
            kv_picks[side][j * BLK : (j + 1) * BLK, :] = kv_all[pl.ds(src, BLK), :]

    def score(i, side):
        kv_pick, s_buf, p_buf = kv_picks[side], s_bufs[side], p_bufs[side]
        r = r_ref[i]
        for c in range(keys // chunk):
            both = lax.dot_general(
                kv_pick[c * chunk : (c + 1) * chunk, :], r, (((1,), (1,)), ((), ())), preferred_element_type=F32
            )
            p_buf[c * chunk : (c + 1) * chunk, :] = both[:, rows:]
            for j in range(4):
                pick = c * 4 + j
                s = both[j * BLK : (j + 1) * BLK, :rows] * LOG2E
                if pick == 0:
                    s = jnp.where(diag, s, -jnp.inf)
                else:
                    bias = jnp.where(acc_loc[i, pick] == dummy, -jnp.inf, 0.0).astype(F32)
                    s = s + bias
                s_buf[pick * BLK : (pick + 1) * BLK, :] = s
            yield

    def weigh(side):
        s_buf, p_buf, x_buf = s_bufs[side], p_bufs[side], x_bufs[side]
        top = jnp.full((8, rows), -jnp.inf, F32)
        for j in range(picks):
            top = jnp.maximum(top, fold(s_buf[j * BLK : (j + 1) * BLK, :], jnp.maximum))
            yield 1
        top = jnp.max(top, axis=0, keepdims=True)
        total = jnp.zeros((8, rows), F32)
        for j in range(picks):
            e = jnp.exp2(s_buf[j * BLK : (j + 1) * BLK, :] - top)
            total = total + fold(e, jnp.add)
            yield 3
        shift = top + jnp.log2(jnp.sum(total, axis=0, keepdims=True))
        dot = jnp.zeros((8, rows), F32)
        for j in range(picks):
            at = slice(j * BLK, (j + 1) * BLK)
            w = jnp.exp2(s_buf[at, :] - shift)
            wb = w.astype(BF)
            s_buf[at, :] = w
            x_buf[at, rows:] = wb
            dot = dot + fold(wb.astype(F32) * p_buf[at, :], jnp.add)
            yield 6
        dot = jnp.sum(dot, axis=0, keepdims=True)
        for j in range(picks):
            at = slice(j * BLK, (j + 1) * BLK)
            x_buf[at, :rows] = (s_buf[at, :] * (p_buf[at, :] - dot)).astype(BF)
            yield 3

    def spread(i, side):
        kv_pick, x_buf = kv_picks[side], x_bufs[side]
        r = r_ref[i]
        dqt = jnp.zeros((width, rows), F32)
        for c in range(keys // chunk):
            at = slice(c * chunk, (c + 1) * chunk)
            x = x_buf[at, :]
            grads = lax.dot_general(x, r, (((1,), (0,)), ((), ())), preferred_element_type=F32)
            for j in range(4):
                dst = pl.multiple_of(acc_loc[i, c * 4 + j] * BLK, BLK)
                acc[pl.ds(dst, BLK), :] += grads[j * BLK : (j + 1) * BLK, :]
            dqt = dqt + lax.dot_general(
                kv_pick[at, :], x[:, :rows], (((0,), (0,)), ((), ())), preferred_element_type=F32
            )
            yield
        dq_buf[...] = dqt[:hd, :] * scale
        row_at = pl.ds(pl.multiple_of(i * BLK, BLK), BLK)
        for pair in range(heads // 2):
            two = jnp.concatenate(
                [dq_buf[:, 2 * pair * BLK : (2 * pair + 1) * BLK], dq_buf[:, (2 * pair + 1) * BLK : (2 * pair + 2) * BLK]],
                axis=0,
            )
            dq_ref[row_at, pair * width : (pair + 1) * width] = two.T.astype(BF)
        yield

    def drain(steps):
        for _ in steps:
            pass

    def turn(i, side):
        other = 1 - side
        after = jnp.minimum(i + 1, nblk - 1)

        def matmuls():
            yield from spread(jnp.maximum(i - 1, 0), other)
            gather(after, other)
            yield from score(after, other)

        pending = matmuls()
        parts = 2 * (keys // chunk) + 1
        whole = 13 * picks
        done = taken = 0
        for units in weigh(side):
            done += units
            while taken < parts and done * parts >= (taken + 1) * whole * 0.9:
                next(pending)
                taken += 1
        drain(pending)

    gather(0, 0)
    drain(score(0, 0))

    def step(i, carry):
        @pl.when(i % 2 == 0)
        def _():
            turn(i, 0)

        @pl.when(i % 2 == 1)
        def _():
            turn(i, 1)

        return carry

    lax.fori_loop(0, nblk, step, 0)
    drain(spread(nblk - 1, 1))
    own_ref[...] = acc[0 : nblk * BLK, :]
    lane = lax.broadcasted_iota(jnp.int32, (LABEL_ROWS, width), 0)
    for h in range(n):
        lo = (nblk + h * slots) * BLK
        out_ref[h, 0 : slots * BLK, :] = acc[lo : lo + slots * BLK, :].astype(BF)
        mark = jnp.zeros((LABEL_ROWS, width), F32)
        for k in range(slots):
            lab = table[0, (k % MOST) * n * seqs + h * seqs + k // MOST]
            mark = jnp.where(lane == k, lab.astype(F32), mark)
        out_ref[h, slots * BLK : slots * BLK + LABEL_ROWS, :] = mark.astype(BF)


def combine_kernel(n, seqs, bpd, hd, parts, quarter, own_ref, msgs, *refs):
    sources = refs[:parts]
    kg_ref, vg_ref, out_ref, total, vbuf, pieces, sems = refs[parts:]
    cut = sources[0].shape[1] // CUTS
    copies = [
        [
            pltpu.make_async_copy(
                sources[j].at[:, pl.ds(q * cut, cut)], pieces.at[j, :, pl.ds(q * cut, cut)], sems.at[j, q]
            )
            for j in range(parts)
        ]
        for q in range(CUTS)
    ]
    for group in copies:
        for copy in group:
            copy.start()
    slots = seqs * MOST
    total[...] = own_ref[...]
    for d in range(n):
        marks = msgs[d, slots * BLK : slots * BLK + LABEL_ROWS, :].astype(F32)
        for s in range(seqs):
            for m in range(MOST):
                k = s * MOST + m
                val = msgs[d, k * BLK : (k + 1) * BLK, :].astype(F32)
                mark = marks[k : k + 1, :]
                for b in range(bpd):
                    at = slice((s * bpd + b) * BLK, (s * bpd + b + 1) * BLK)
                    total[at, :] = total[at, :] + jnp.where(mark == float(b), val, 0.0)
    tok = bpd * BLK
    kg_ref[...] = total[:, :hd].astype(BF)
    vg = total[:, hd:].astype(BF)
    vg_ref[...] = vg
    vbuf[...] = vg
    span = tok // parts
    turned = []
    for j in range(parts):
        who = jnp.bitwise_xor(quarter[0], j)
        v = [
            vbuf[pl.ds(pl.multiple_of(s * tok + who * span, 16), span), :].astype(F32)
            for s in range(seqs)
        ]
        turned.append(jnp.concatenate(v, axis=0).T.astype(BF))
    lanes = out_ref.shape[2]
    for i in range(out_ref.shape[0] // 2):
        if (2 * i * lanes) % cut == 0:
            for copy in copies[2 * i * lanes // cut]:
                copy.wait()
        acc = jnp.zeros((hd, 2 * lanes), F32)
        for j in range(parts):
            x = pieces[j, :, 2 * i * lanes : 2 * (i + 1) * lanes]
            acc = acc + jnp.dot(turned[j], x, preferred_element_type=F32)
        out_ref[2 * i] = acc[:, :lanes].astype(BF)
        out_ref[2 * i + 1] = acc[:, lanes:].astype(BF)


def final_kernel(n, parts, in_ref, out_ref):
    for t in range(parts):
        acc = in_ref[t].astype(F32)
        for k in range(1, n):
            acc = acc + in_ref[k * parts + t].astype(F32)
        if t % 2 == 0:
            held = acc
        else:
            both = jnp.concatenate([held, acc], axis=0)
            w = both.shape[0]
            out_ref[:, (t // 2) * w : (t // 2 + 1) * w] = both.T


def on_device(queries, key_states, value_states, cotangent, gate_logits, layer_input, chosen):
    seqs, tok, row_width = queries.shape
    hd = key_states.shape[2]
    heads = row_width // hd
    bpd = tok // BLK
    picks = chosen.shape[3]
    pairs = lax.axis_size("hi")
    n = 2 * pairs
    parts = lax.axis_size("tp")
    own = lax.axis_index(KV).astype(jnp.int32)
    t_own = lax.axis_index("tp").astype(jnp.int32)
    scale = hd ** (-0.5)
    assert math.log2(scale).is_integer() and n % 2 == 0
    nblk = seqs * bpd
    slots = seqs * MOST
    zshifts = pairs - 1
    width = 2 * hd

    perm = lax.ppermute
    own_at = own.reshape(1)
    lanes = -(-MOST * n * seqs // 128) * 128
    kv, table = pl.pallas_call(
        functools.partial(front_kernel, n, seqs, bpd),
        out_shape=[
            jax.ShapeDtypeStruct((seqs * tok, width), BF),
            jax.ShapeDtypeStruct((1, lanes), jnp.int32),
        ],
        in_specs=[vspec()] * 3,
        out_specs=[vspec()] * 2,
        compiler_params=grant(3),
        name="front",
    )(chosen, key_states.transpose(0, 2, 1), value_states.transpose(0, 2, 1))
    perm = lax.ppermute
    partner = perm(kv, "lo", [(0, 1), (1, 0)])

    asked = [
        perm(table, "hi", [(k, k - d) for k in range(d, pairs)]) for d in range(1, pairs)
    ]

    tp_xor = lambda j: [(i, i ^ j) for i in range(parts)]
    mine = layer_input.reshape(seqs * layer_input.shape[1], layer_input.shape[2])
    piece2 = perm(mine, "tp", tp_xor(2))
    piece1 = perm(mine, "tp", tp_xor(1))

    prepare = pl.pallas_call(
        functools.partial(prep_kernel, n, seqs, bpd, heads, hd, scale),
        out_shape=[
            jax.ShapeDtypeStruct((nblk, 2 * heads * BLK, width), BF),
            jax.ShapeDtypeStruct((nblk, picks), jnp.int32),
            jax.ShapeDtypeStruct((nblk, picks), jnp.int32),
        ],
        in_specs=[sspec()] * 2 + [vspec()] * 4,
        out_specs=[vspec()] * 3,
        scratch_shapes=[VMEM((seqs * tok, heads), F32)],
        compiler_params=grant(3),
        name="prep",
    )
    r, kv_loc, acc_loc = prepare(
        table,
        own_at,
        chosen,
        gate_logits.transpose(0, 2, 1),
        queries.reshape(seqs * tok, row_width),
        cotangent.reshape(seqs * tok, row_width),
    )

    zrows = slots * 2 * BLK
    packed = pl.pallas_call(
        functools.partial(pack_kernel, seqs, bpd, n, zshifts),
        out_shape=[jax.ShapeDtypeStruct((zrows, width), BF)] * zshifts,
        in_specs=[sspec()] * (zshifts + 1) + [vspec()] * 2,
        out_specs=[vspec()] * zshifts,
        scratch_shapes=[VMEM((2 * nblk * BLK, width), BF)],
        compiler_params=grant(3),
        name="pack",
    )(*asked, own_at, kv, partner)
    far = [
        perm(packed[d - 1], "hi", [(k, k + d) for k in range(pairs - d)]) for d in range(1, pairs)
    ]
    dummy = nblk + n * slots

    keys = picks * BLK
    rows = heads * BLK
    mrows = slots * BLK + LABEL_ROWS
    attended = pl.pallas_call(
        functools.partial(attend_kernel, n, nblk, bpd, heads, hd, picks, scale),
        out_shape=[
            jax.ShapeDtypeStruct((seqs * tok, row_width), BF),
            jax.ShapeDtypeStruct((nblk * BLK, width), F32),
            jax.ShapeDtypeStruct((n, mrows, width), BF),
        ],
        in_specs=[sspec()] * 3 + [vspec()] * (3 + zshifts),
        out_specs=[vspec()] * 3,
        scratch_shapes=[
            VMEM((2 * nblk * BLK + zshifts * zrows, width), BF),
            VMEM(((dummy + 1) * BLK, width), F32),
            VMEM((hd, rows), F32),
        ]
        + [VMEM((keys, width), BF)] * 2
        + [VMEM((keys, rows), F32)] * 4
        + [VMEM((keys, 2 * rows), BF)] * 2,
        compiler_params=grant(14),
        name="attend",
    )(kv_loc, acc_loc, table, r, kv, partner, *far)
    query_grad = attended[0].reshape(seqs, tok, row_width)
    arrived = lax.all_to_all(attended[2], KV, split_axis=0, concat_axis=0, tiled=True)
    own_sum, piece2 = lax.optimization_barrier((attended[1], piece2))
    piece3 = perm(piece2, "tp", tp_xor(1))
    pieces = [mine, piece1, piece2, piece3]

    ranks = n * parts
    depth = layer_input.shape[2]
    share = depth // ranks
    kg, vg, partial = pl.pallas_call(
        functools.partial(combine_kernel, n, seqs, bpd, hd, parts),
        out_shape=[
            jax.ShapeDtypeStruct((seqs * tok, hd), BF),
            jax.ShapeDtypeStruct((seqs * tok, hd), BF),
            jax.ShapeDtypeStruct((ranks * share // 128, hd, 128), BF),
        ],
        in_specs=[sspec()] + [vspec()] * 2 + [pl.BlockSpec(memory_space=pl.ANY)] * parts,
        out_specs=[vspec()] * 3,
        scratch_shapes=[
            VMEM((nblk * BLK, width), F32),
            VMEM((seqs * tok, hd), BF),
            VMEM((parts,) + mine.shape, BF),
            pltpu.SemaphoreType.DMA((parts, CUTS)),
        ],
        compiler_params=grant(10),
        name="combine",
    )(t_own.reshape(1), own_sum, arrived, *pieces)
    key_grad = kg.reshape(seqs, tok, hd)
    value_grad = vg.reshape(seqs, tok, hd)
    if share != 128:
        partial = partial.transpose(1, 0, 2).reshape(hd, ranks, share).transpose(1, 0, 2)
    swapped = lax.all_to_all(partial, KV + ("tp",), split_axis=0, concat_axis=0, tiled=True)
    value_weight_grad = pl.pallas_call(
        functools.partial(final_kernel, n, parts),
        out_shape=jax.ShapeDtypeStruct((share, parts * hd), F32),
        in_specs=[vspec()],
        out_specs=vspec(),
        compiler_params=grant(2),
        name="final",
    )(swapped)
    return query_grad, key_grad, value_grad, value_weight_grad


def solution(mesh):
    count = mesh.shape["kv"]
    split = jax.sharding.Mesh(
        mesh.devices.reshape(count // 2, 2, mesh.shape["tp"]), ("hi", "lo", "tp")
    )
    in_specs = (
        P(None, KV, "tp"),
        P(None, KV, "tp"),
        P(None, KV, "tp"),
        P(None, KV, "tp"),
        P(None, KV, "tp"),
        P(None, KV + ("tp",), None),
        P(None, KV, "tp", None),
    )
    out_specs = (
        P(None, KV, "tp"),
        P(None, KV, "tp"),
        P(None, KV, "tp"),
        P(KV + ("tp",), None),
    )

    return jax.shard_map(
        on_device, mesh=split, in_specs=in_specs, out_specs=out_specs, check_vma=False
    )
```

```python
import functools
import math

import jax
import jax.numpy as jnp
from jax import lax
from jax.experimental import pallas as pl
from jax.experimental.pallas import tpu as pltpu
from jax.sharding import PartitionSpec as P


BLK = 64
MOST = 2
LABEL_ROWS = 8
CUTS = 4
LOG2E = math.log2(math.e)
KV = ("hi", "lo")
BF = jnp.bfloat16
F32 = jnp.float32
VMEM = pltpu.VMEM
SMEM = pltpu.SMEM
MIB = 1024 * 1024


def grant(mib):
    return pltpu.CompilerParams(vmem_limit_bytes=mib * MIB)


def vspec():
    return pl.BlockSpec(memory_space=VMEM)


def hspec():
    return pl.BlockSpec(memory_space=pltpu.HBM)


def stay(x):
    return pltpu.with_memory_space_constraint(x, pltpu.HBM)


def sspec():
    return pl.BlockSpec(memory_space=SMEM)


def bring(pairs, sems):
    copies = [pltpu.make_async_copy(a, b, sems.at[k]) for k, (a, b) in enumerate(pairs)]
    for copy in copies:
        copy.start()
    return copies


def front_kernel(
    n, seqs, bpd, ids_hbm, key_hbm, value_hbm, kv_ref, table_ref, ids_ref, key_ref, value_ref, sems
):
    tok = key_ref.shape[2]
    for copy in bring([(ids_hbm, ids_ref), (key_hbm, key_ref), (value_hbm, value_ref)], sems):
        copy.wait()
    for s in range(seqs):
        both = jnp.concatenate([key_ref[s], value_ref[s]], axis=0).astype(F32)
        kv_ref[s * tok : (s + 1) * tok, :] = both.T.astype(BF)
    lane = lax.broadcasted_iota(jnp.int32, table_ref.shape, 1)
    table = jnp.zeros(table_ref.shape, jnp.int32)
    for s in range(seqs):
        c = ids_ref[s, :, 0, :]
        h = lax.shift_right_logical(c * -(-(1 << 20) // bpd), 20)
        w = c - h * bpd
        for k in range(n):
            low = jnp.min(jnp.where(h == k, w, bpd - 1).astype(F32), keepdims=True)
            high = jnp.max(jnp.where(h == k, w, 0).astype(F32), keepdims=True)
            table = jnp.where(lane == k * seqs + s, low.astype(jnp.int32), table)
            table = jnp.where(lane == (n + k) * seqs + s, high.astype(jnp.int32), table)
    table_ref[...] = table


def prep_kernel(
    n,
    seqs,
    bpd,
    heads,
    hd,
    scale,
    table,
    own_ref,
    ids_hbm,
    gate_hbm,
    q_hbm,
    g_hbm,
    r_ref,
    kv_loc,
    acc_loc,
    ids,
    gate_ref,
    q_ref,
    g_ref,
    gate_buf,
    sems,
):
    width = 2 * hd
    rows = heads * BLK
    copies = bring([(ids_hbm, ids), (gate_hbm, gate_ref), (q_hbm, q_ref), (g_hbm, g_ref)], sems)
    for copy in copies[:2]:
        copy.wait()
    tok = bpd * BLK
    for s in range(seqs):
        gate_buf[s * tok : (s + 1) * tok, :] = jax.nn.sigmoid(gate_ref[s]).T
    front = lax.broadcasted_iota(jnp.int32, (BLK, width), 1) < hd

    def step(i, carry):
        at = pl.ds(pl.multiple_of(i * BLK, BLK), BLK)
        gates = gate_buf[at, :]
        for pair in range(heads // 2):
            q = q_ref[at, pair * width : (pair + 1) * width].astype(F32) * scale
            g = g_ref[at, pair * width : (pair + 1) * width].astype(F32)
            gv = jnp.where(front, gates[:, 2 * pair : 2 * pair + 1], gates[:, 2 * pair + 1 : 2 * pair + 2])
            g = g * gv
            qr = pltpu.roll(q, hd, 1)
            gr = pltpu.roll(g, hd, 1)
            zero = jnp.zeros_like(q)
            base = 2 * pair * BLK
            r_ref[i, base : base + BLK, :] = jnp.where(front, q, zero).astype(BF)
            r_ref[i, base + BLK : base + 2 * BLK, :] = jnp.where(front, qr, zero).astype(BF)
            r_ref[i, rows + base : rows + base + BLK, :] = jnp.where(front, zero, gr).astype(BF)
            r_ref[i, rows + base + BLK : rows + base + 2 * BLK, :] = jnp.where(front, zero, g).astype(BF)
        return carry

    nblk = seqs * bpd
    own = own_ref[0]
    dummy = nblk + n * seqs * MOST
    named = jnp.concatenate([ids[s, :, 0, :] for s in range(seqs)], axis=0)
    row = lax.broadcasted_iota(jnp.int32, named.shape, 0)
    start = lax.broadcasted_iota(jnp.int32, named.shape, 1) == 0
    s = jnp.zeros_like(row)
    for k in range(1, seqs):
        s = s + (row >= k * bpd).astype(jnp.int32)
    block = own * bpd + row - s * bpd
    c = jnp.where(start, block, jnp.where(named == block, named[:, 0:1], named))
    h = lax.shift_right_logical(c * -(-(1 << 20) // bpd), 20)
    w = c - h * bpd
    low = jnp.zeros_like(c)
    for k in range(n):
        here = jnp.full_like(c, table[0, k * seqs])
        for q in range(1, seqs):
            here = jnp.where(s == q, table[0, k * seqs + q], here)
        low = jnp.where(h == k, here, low)
    slot = (w != low).astype(jnp.int32)
    own_z = lax.shift_right_logical(own, 1)
    h_z = lax.shift_right_logical(h, 1)
    home = s * bpd + w
    far = 2 * nblk + (((own_z - h_z - 1) * seqs + s) * 2 + (h & 1)) * MOST + slot
    near = jnp.where(h == own, home, nblk + home)
    future = c > block
    kv_loc[...] = jnp.where(future, 0, jnp.where(h_z == own_z, near, far))
    remote = nblk + (h * seqs + s) * MOST + slot
    acc_loc[...] = jnp.where(future, dummy, jnp.where(h == own, home, remote))

    for copy in copies[2:]:
        copy.wait()
    lax.fori_loop(0, nblk, step, 0)


def pack_kernel(seqs, bpd, n, shifts, *refs):
    tables = refs[:shifts]
    own_ref, kv_ref, partner_ref = refs[shifts : shifts + 3]
    outs = refs[shifts + 3 : 2 * shifts + 3]
    both = refs[2 * shifts + 3]
    rows = kv_ref.shape[0]
    both[0:rows, :] = kv_ref[...]
    both[rows : 2 * rows, :] = partner_ref[...]
    own = own_ref[0]
    side = own & 1
    for d in range(shifts):
        for s in range(seqs):
            for yh in range(2):
                for m in range(MOST):
                    slot = (s * 2 + yh) * MOST + m
                    lab = tables[d][0, m * n * seqs + (own - side + yh) * seqs + s]
                    at = ((side ^ yh) * seqs + s) * bpd + lab
                    src = pl.multiple_of(at * BLK, BLK)
                    outs[d][slot * BLK : (slot + 1) * BLK, :] = both[pl.ds(src, BLK), :]


def attend_kernel(
    n,
    nblk,
    bpd,
    heads,
    hd,
    picks,
    scale,
    kv_loc,
    acc_loc,
    table,
    r_ref,
    kv_ref,
    partner_ref,
    *refs,
):
    zshifts = n // 2 - 1
    far = refs[:zshifts]
    dq_ref, own_ref, out_ref, kv_all, acc, dq_buf = refs[zshifts : zshifts + 6]
    sets = refs[zshifts + 6 :]
    kv_picks, s_bufs, p_bufs, x_bufs = sets[0:2], sets[2:4], sets[4:6], sets[6:8]
    rows = heads * BLK
    width = 2 * hd
    seqs = nblk // bpd
    slots = seqs * MOST
    dummy = nblk + n * slots
    chunk = 4 * BLK
    keys = picks * BLK

    pair_rows = 2 * nblk * BLK
    kv_all[0 : nblk * BLK, :] = kv_ref[...]
    kv_all[nblk * BLK : pair_rows, :] = partner_ref[...]
    for d in range(zshifts):
        span = far[d].shape[0]
        kv_all[pair_rows + d * span : pair_rows + (d + 1) * span, :] = far[d][...]
    acc[...] = jnp.zeros_like(acc)
    x_bufs[1][...] = jnp.zeros_like(x_bufs[1])
    kv_picks[1][...] = jnp.zeros_like(kv_picks[1])
    kpos = lax.broadcasted_iota(jnp.int32, (BLK, rows), 0)
    qpos = lax.broadcasted_iota(jnp.int32, (BLK, rows), 1) % BLK
    diag = kpos <= qpos

    def fold(x, op):
        out = x[0:8, :]
        for i in range(1, x.shape[0] // 8):
            out = op(out, x[i * 8 : (i + 1) * 8, :])
        return out

    def gather(i, side):
        for j in range(picks):
            src = pl.multiple_of(kv_loc[i, j] * BLK, BLK)
            kv_picks[side][j * BLK : (j + 1) * BLK, :] = kv_all[pl.ds(src, BLK), :]

    def score(i, side):
        kv_pick, s_buf, p_buf = kv_picks[side], s_bufs[side], p_bufs[side]
        r = r_ref[i]
        for c in range(keys // chunk):
            both = lax.dot_general(
                kv_pick[c * chunk : (c + 1) * chunk, :], r, (((1,), (1,)), ((), ())), preferred_element_type=F32
            )
            p_buf[c * chunk : (c + 1) * chunk, :] = both[:, rows:]
            for j in range(4):
                pick = c * 4 + j
                s = both[j * BLK : (j + 1) * BLK, :rows] * LOG2E
                if pick == 0:
                    s = jnp.where(diag, s, -jnp.inf)
                else:
                    bias = jnp.where(acc_loc[i, pick] == dummy, -jnp.inf, 0.0).astype(F32)
                    s = s + bias
                s_buf[pick * BLK : (pick + 1) * BLK, :] = s
            yield

    def weigh(side):
        s_buf, p_buf, x_buf = s_bufs[side], p_bufs[side], x_bufs[side]
        top = jnp.full((8, rows), -jnp.inf, F32)
        for j in range(picks):
            top = jnp.maximum(top, fold(s_buf[j * BLK : (j + 1) * BLK, :], jnp.maximum))
            yield 1
        top = jnp.max(top, axis=0, keepdims=True)
        total = jnp.zeros((8, rows), F32)
        for j in range(picks):
            e = jnp.exp2(s_buf[j * BLK : (j + 1) * BLK, :] - top)
            total = total + fold(e, jnp.add)
            yield 3
        shift = top + jnp.log2(jnp.sum(total, axis=0, keepdims=True))
        dot = jnp.zeros((8, rows), F32)
        for j in range(picks):
            at = slice(j * BLK, (j + 1) * BLK)
            w = jnp.exp2(s_buf[at, :] - shift)
            wb = w.astype(BF)
            s_buf[at, :] = w
            x_buf[at, rows:] = wb
            dot = dot + fold(wb.astype(F32) * p_buf[at, :], jnp.add)
            yield 6
        dot = jnp.sum(dot, axis=0, keepdims=True)
        for j in range(picks):
            at = slice(j * BLK, (j + 1) * BLK)
            x_buf[at, :rows] = (s_buf[at, :] * (p_buf[at, :] - dot)).astype(BF)
            yield 3

    def spread(i, side):
        kv_pick, x_buf = kv_picks[side], x_bufs[side]
        r = r_ref[i]
        dqt = jnp.zeros((width, rows), F32)
        for c in range(keys // chunk):
            at = slice(c * chunk, (c + 1) * chunk)
            x = x_buf[at, :]
            grads = lax.dot_general(x, r, (((1,), (0,)), ((), ())), preferred_element_type=F32)
            for j in range(4):
                dst = pl.multiple_of(acc_loc[i, c * 4 + j] * BLK, BLK)
                acc[pl.ds(dst, BLK), :] += grads[j * BLK : (j + 1) * BLK, :]
            dqt = dqt + lax.dot_general(
                kv_pick[at, :], x[:, :rows], (((0,), (0,)), ((), ())), preferred_element_type=F32
            )
            yield
        dq_buf[...] = dqt[:hd, :] * scale
        row_at = pl.ds(pl.multiple_of(i * BLK, BLK), BLK)
        for pair in range(heads // 2):
            two = jnp.concatenate(
                [dq_buf[:, 2 * pair * BLK : (2 * pair + 1) * BLK], dq_buf[:, (2 * pair + 1) * BLK : (2 * pair + 2) * BLK]],
                axis=0,
            )
            dq_ref[row_at, pair * width : (pair + 1) * width] = two.T.astype(BF)
        yield

    def drain(steps):
        for _ in steps:
            pass

    def turn(i, side):
        other = 1 - side
        after = jnp.minimum(i + 1, nblk - 1)

        def matmuls():
            yield from spread(jnp.maximum(i - 1, 0), other)
            gather(after, other)
            yield from score(after, other)

        pending = matmuls()
        parts = 2 * (keys // chunk) + 1
        whole = 13 * picks
        done = taken = 0
        for units in weigh(side):
            done += units
            while taken < parts and done * parts >= (taken + 1) * whole * 0.8:
                next(pending)
                taken += 1
        drain(pending)

    gather(0, 0)
    drain(score(0, 0))

    def step(i, carry):
        @pl.when(i % 2 == 0)
        def _():
            turn(i, 0)

        @pl.when(i % 2 == 1)
        def _():
            turn(i, 1)

        return carry

    lax.fori_loop(0, nblk, step, 0)
    drain(spread(nblk - 1, 1))
    own_ref[...] = acc[0 : nblk * BLK, :]
    lane = lax.broadcasted_iota(jnp.int32, (LABEL_ROWS, width), 0)
    for h in range(n):
        lo = (nblk + h * slots) * BLK
        out_ref[h, 0 : slots * BLK, :] = acc[lo : lo + slots * BLK, :].astype(BF)
        mark = jnp.zeros((LABEL_ROWS, width), F32)
        for k in range(slots):
            lab = table[0, (k % MOST) * n * seqs + h * seqs + k // MOST]
            mark = jnp.where(lane == k, lab.astype(F32), mark)
        out_ref[h, slots * BLK : slots * BLK + LABEL_ROWS, :] = mark.astype(BF)


def combine_kernel(n, seqs, bpd, hd, parts, quarter, own_ref, msgs, *refs):
    sources = refs[:parts]
    kg_ref, vg_ref, out_ref, total, vbuf, pieces, sems = refs[parts:]
    cut = sources[0].shape[1] // CUTS
    copies = [
        [
            pltpu.make_async_copy(
                sources[j].at[:, pl.ds(q * cut, cut)], pieces.at[j, :, pl.ds(q * cut, cut)], sems.at[j, q]
            )
            for j in range(parts)
        ]
        for q in range(CUTS)
    ]
    for group in copies:
        for copy in group:
            copy.start()
    slots = seqs * MOST
    total[...] = own_ref[...]
    for d in range(n):
        marks = msgs[d, slots * BLK : slots * BLK + LABEL_ROWS, :].astype(F32)
        for s in range(seqs):
            for m in range(MOST):
                k = s * MOST + m
                val = msgs[d, k * BLK : (k + 1) * BLK, :].astype(F32)
                mark = marks[k : k + 1, :]
                for b in range(bpd):
                    at = slice((s * bpd + b) * BLK, (s * bpd + b + 1) * BLK)
                    total[at, :] = total[at, :] + jnp.where(mark == float(b), val, 0.0)
    tok = bpd * BLK
    kg_ref[...] = total[:, :hd].astype(BF)
    vg = total[:, hd:].astype(BF)
    vg_ref[...] = vg
    vbuf[...] = vg
    span = tok // parts
    turned = []
    for j in range(parts):
        who = jnp.bitwise_xor(quarter[0], j)
        v = [
            vbuf[pl.ds(pl.multiple_of(s * tok + who * span, 16), span), :].astype(F32)
            for s in range(seqs)
        ]
        turned.append(jnp.concatenate(v, axis=0).T.astype(BF))
    lanes = out_ref.shape[2]
    for i in range(out_ref.shape[0] // 2):
        if (2 * i * lanes) % cut == 0:
            for copy in copies[2 * i * lanes // cut]:
                copy.wait()
        acc = jnp.zeros((hd, 2 * lanes), F32)
        for j in range(parts):
            x = pieces[j, :, 2 * i * lanes : 2 * (i + 1) * lanes]
            acc = acc + jnp.dot(turned[j], x, preferred_element_type=F32)
        out_ref[2 * i] = acc[:, :lanes].astype(BF)
        out_ref[2 * i + 1] = acc[:, lanes:].astype(BF)


def final_kernel(n, parts, in_ref, out_ref):
    for t in range(parts):
        acc = in_ref[t].astype(F32)
        for k in range(1, n):
            acc = acc + in_ref[k * parts + t].astype(F32)
        if t % 2 == 0:
            held = acc
        else:
            both = jnp.concatenate([held, acc], axis=0)
            w = both.shape[0]
            out_ref[:, (t // 2) * w : (t // 2 + 1) * w] = both.T


def on_device(queries, key_states, value_states, cotangent, gate_logits, layer_input, chosen):
    seqs, tok, row_width = queries.shape
    hd = key_states.shape[2]
    heads = row_width // hd
    bpd = tok // BLK
    picks = chosen.shape[3]
    pairs = lax.axis_size("hi")
    n = 2 * pairs
    parts = lax.axis_size("tp")
    own = lax.axis_index(KV).astype(jnp.int32)
    t_own = lax.axis_index("tp").astype(jnp.int32)
    scale = hd ** (-0.5)
    assert math.log2(scale).is_integer() and n % 2 == 0
    nblk = seqs * bpd
    slots = seqs * MOST
    zshifts = pairs - 1
    width = 2 * hd

    perm = lax.ppermute
    own_at = own.reshape(1)
    lanes = -(-MOST * n * seqs // 128) * 128
    kv, table = pl.pallas_call(
        functools.partial(front_kernel, n, seqs, bpd),
        out_shape=[
            jax.ShapeDtypeStruct((seqs * tok, width), BF),
            jax.ShapeDtypeStruct((1, lanes), jnp.int32),
        ],
        in_specs=[hspec()] * 3,
        out_specs=[vspec()] * 2,
        scratch_shapes=[
            VMEM(chosen.shape, jnp.int32),
            VMEM((seqs, hd, tok), BF),
            VMEM((seqs, hd, tok), BF),
            pltpu.SemaphoreType.DMA((3,)),
        ],
        compiler_params=grant(3),
        name="front",
    )(stay(chosen), stay(key_states.transpose(0, 2, 1)), stay(value_states.transpose(0, 2, 1)))
    perm = lax.ppermute
    partner = perm(kv, "lo", [(0, 1), (1, 0)])

    asked = [
        perm(table, "hi", [(k, k - d) for k in range(d, pairs)]) for d in range(1, pairs)
    ]

    tp_xor = lambda j: [(i, i ^ j) for i in range(parts)]
    mine = layer_input.reshape(seqs * layer_input.shape[1], layer_input.shape[2])
    piece2 = perm(mine, "tp", tp_xor(2))
    piece1 = perm(mine, "tp", tp_xor(1))

    prepare = pl.pallas_call(
        functools.partial(prep_kernel, n, seqs, bpd, heads, hd, scale),
        out_shape=[
            jax.ShapeDtypeStruct((nblk, 2 * heads * BLK, width), BF),
            jax.ShapeDtypeStruct((nblk, picks), jnp.int32),
            jax.ShapeDtypeStruct((nblk, picks), jnp.int32),
        ],
        in_specs=[sspec()] * 2 + [hspec()] * 4,
        out_specs=[vspec()] * 3,
        scratch_shapes=[
            VMEM(chosen.shape, jnp.int32),
            VMEM((seqs, heads, tok), F32),
            VMEM((seqs * tok, row_width), BF),
            VMEM((seqs * tok, row_width), BF),
            VMEM((seqs * tok, heads), F32),
            pltpu.SemaphoreType.DMA((4,)),
        ],
        compiler_params=grant(5),
        name="prep",
    )
    r, kv_loc, acc_loc = prepare(
        table,
        own_at,
        stay(chosen),
        stay(gate_logits.transpose(0, 2, 1)),
        stay(queries.reshape(seqs * tok, row_width)),
        stay(cotangent.reshape(seqs * tok, row_width)),
    )

    zrows = slots * 2 * BLK
    packed = pl.pallas_call(
        functools.partial(pack_kernel, seqs, bpd, n, zshifts),
        out_shape=[jax.ShapeDtypeStruct((zrows, width), BF)] * zshifts,
        in_specs=[sspec()] * (zshifts + 1) + [vspec()] * 2,
        out_specs=[vspec()] * zshifts,
        scratch_shapes=[VMEM((2 * nblk * BLK, width), BF)],
        compiler_params=grant(3),
        name="pack",
    )(*asked, own_at, kv, partner)
    far = [
        perm(packed[d - 1], "hi", [(k, k + d) for k in range(pairs - d)]) for d in range(1, pairs)
    ]
    dummy = nblk + n * slots

    keys = picks * BLK
    rows = heads * BLK
    mrows = slots * BLK + LABEL_ROWS
    attended = pl.pallas_call(
        functools.partial(attend_kernel, n, nblk, bpd, heads, hd, picks, scale),
        out_shape=[
            jax.ShapeDtypeStruct((seqs * tok, row_width), BF),
            jax.ShapeDtypeStruct((nblk * BLK, width), F32),
            jax.ShapeDtypeStruct((n, mrows, width), BF),
        ],
        in_specs=[sspec()] * 3 + [vspec()] * (3 + zshifts),
        out_specs=[vspec()] * 3,
        scratch_shapes=[
            VMEM((2 * nblk * BLK + zshifts * zrows, width), BF),
            VMEM(((dummy + 1) * BLK, width), F32),
            VMEM((hd, rows), F32),
        ]
        + [VMEM((keys, width), BF)] * 2
        + [VMEM((keys, rows), F32)] * 4
        + [VMEM((keys, 2 * rows), BF)] * 2,
        compiler_params=grant(14),
        name="attend",
    )(kv_loc, acc_loc, table, r, kv, partner, *far)
    query_grad = attended[0].reshape(seqs, tok, row_width)
    arrived = lax.all_to_all(attended[2], KV, split_axis=0, concat_axis=0, tiled=True)
    own_sum, piece2 = lax.optimization_barrier((attended[1], piece2))
    piece3 = perm(piece2, "tp", tp_xor(1))
    pieces = [mine, piece1, piece2, piece3]

    ranks = n * parts
    depth = layer_input.shape[2]
    share = depth // ranks
    kg, vg, partial = pl.pallas_call(
        functools.partial(combine_kernel, n, seqs, bpd, hd, parts),
        out_shape=[
            jax.ShapeDtypeStruct((seqs * tok, hd), BF),
            jax.ShapeDtypeStruct((seqs * tok, hd), BF),
            jax.ShapeDtypeStruct((ranks * share // 128, hd, 128), BF),
        ],
        in_specs=[sspec()] + [vspec()] * 2 + [pl.BlockSpec(memory_space=pl.ANY)] * parts,
        out_specs=[vspec()] * 3,
        scratch_shapes=[
            VMEM((nblk * BLK, width), F32),
            VMEM((seqs * tok, hd), BF),
            VMEM((parts,) + mine.shape, BF),
            pltpu.SemaphoreType.DMA((parts, CUTS)),
        ],
        compiler_params=grant(10),
        name="combine",
    )(t_own.reshape(1), own_sum, arrived, *pieces)
    key_grad = kg.reshape(seqs, tok, hd)
    value_grad = vg.reshape(seqs, tok, hd)
    if share != 128:
        partial = partial.transpose(1, 0, 2).reshape(hd, ranks, share).transpose(1, 0, 2)
    swapped = lax.all_to_all(partial, KV + ("tp",), split_axis=0, concat_axis=0, tiled=True)
    value_weight_grad = pl.pallas_call(
        functools.partial(final_kernel, n, parts),
        out_shape=jax.ShapeDtypeStruct((share, parts * hd), F32),
        in_specs=[vspec()],
        out_specs=vspec(),
        compiler_params=grant(2),
        name="final",
    )(swapped)
    return query_grad, key_grad, value_grad, value_weight_grad


def solution(mesh):
    count = mesh.shape["kv"]
    split = jax.sharding.Mesh(
        mesh.devices.reshape(count // 2, 2, mesh.shape["tp"]), ("hi", "lo", "tp")
    )
    in_specs = (
        P(None, KV, "tp"),
        P(None, KV, "tp"),
        P(None, KV, "tp"),
        P(None, KV, "tp"),
        P(None, KV, "tp"),
        P(None, KV + ("tp",), None),
        P(None, KV, "tp", None),
    )
    out_specs = (
        P(None, KV, "tp"),
        P(None, KV, "tp"),
        P(None, KV, "tp"),
        P(KV + ("tp",), None),
    )

    return jax.shard_map(
        on_device, mesh=split, in_specs=in_specs, out_specs=out_specs, check_vma=False
    )
```
